512 devices in a mesh: grp: 2 (over y), sp: 64 (over z, core), tp: 4 (over x).
Axes of the slice: x: 4, y: 2, z: 32, core: 2. Of those that a mesh axis runs over, the one named last changes fastest.
The devices are a block of a 4x8x32 slice.
Arguments:
- tokens: bfloat16 [32768, 2048], P(('grp', 'sp'), 'tp'), parts along dimension 0, may hold values from -6 to 6
- norm_gain: float32 [2048], replicated, may hold values from 0.1 to 1.9
- ret_query_weight: bfloat16 [2048, 256], P('sp', 'tp'), may hold values from -0.125 to 0.125
- ret_key_weight: bfloat16 [2048, 256], P('sp', 'tp'), may hold values from -0.125 to 0.125
- ret_value_weight: bfloat16 [2048, 512], P('sp', 'tp'), may hold values from -0.125 to 0.125
- fox_query_weight: bfloat16 [2048, 512], P('sp', 'tp'), may hold values from -8 to 8
- fox_key_weight: bfloat16 [2048, 512], P('sp', 'tp'), may hold values from -0.125 to 0.125
- fox_value_weight: bfloat16 [2048, 512], P('sp', 'tp'), may hold values from -0.125 to 0.125
- ret_decay: float32 [8], P('tp'), may hold values from -1 to 0, as said below
- ret_state: float32 [16, 32, 64], P(('grp', 'tp')), parts along dimension 0, may hold values from -256 to 256
- head_norm_gain: float32 [512], P('tp'), may hold values from 0.1 to 1.9
- fox_gates: float32 [32768, 8], P('grp', 'tp'), parts along dimension 0, may hold values from -49152 to 0, as said below
- ret_out_weight: bfloat16 [512, 2048], P('tp', 'sp'), may hold values from -0.1875 to 0.1875
- fox_out_weight: bfloat16 [512, 2048], P('tp', 'sp'), may hold values from -1 to 1
Outputs:
- mixed: bfloat16 [32768, 2048], P(('grp', 'sp', 'tp')), parts along dimension 0
The draws below stay inside these ranges and needn't reach their ends.
There are 2 independent parts, one for each index of `grp`. The reference program is written for one: setup_inputs(seed, part) draws one part's arguments, and reference() takes and returns one part's arrays. A program takes and returns all parts, laid end to end along the dimension named above; an argument that names none is the same for every part. Nothing has to cross between parts.
Inputs may be any that keep to these rules, and one draw needn't show every extreme that they name: `ret_decay`: each head's log decay is negative. `fox_gates`: along the positions each head's column never rises.
All inputs are finite; a program needn't handle non-finite values.
Results may differ from the reference program's by a relative error of at most 0.015.
The reference program's roundings to bfloat16 on the way count: a program that leaves them out, or rounds other values in their place, can miss the bound.
Values may be sent and summed in bfloat16 or wider, within the bound.
A program may use at most 64 MiB of HBM per device.

```python
import jax
import jax.numpy as jnp
from jax import lax

D = 2048
RETAIN_HEADS = 8
DK = 32
RETAIN_VALUE_DIM = 64
FH = 8
FD = 64
TOK_DEV = 256
TOKENS = 16384
N_TP = 4


def draw_fox_query_weight(key, part):
    keys = jax.random.split(jax.random.fold_in(key, 11), 1)
    columns = FH * FD
    return (jnp.clip(jax.random.normal(keys[0], (D, columns), jnp.float32), -6.0, 6.0) * D ** (-0.5)).astype(jnp.bfloat16)


def draw_ret_decay(key, part):
    keys = jax.random.split(jax.random.fold_in(key, 23), 3)
    order = jax.random.permutation(keys[0], RETAIN_HEADS)
    quick = order < RETAIN_HEADS // 2
    quick_rate = -1.0 / jax.random.uniform(keys[1], (RETAIN_HEADS,), jnp.float32, 30.0, 100.0)
    slow_rate = -jax.random.uniform(keys[2], (RETAIN_HEADS,), jnp.float32, 0.3, 2.0) / TOKENS
    return jnp.where(quick, quick_rate, slow_rate)


def draw_ret_state(key, part):
    source = jax.random.fold_in(key, 37)
    scale = 0.2 * float(TOKENS) ** 0.5
    return scale * jnp.clip(jax.random.normal(source, (RETAIN_HEADS, DK, RETAIN_VALUE_DIM), jnp.float32), -6.0, 6.0)


def draw_fox_gates(key, part):
    keys = jax.random.split(jax.random.fold_in(key, 51), 7)
    order = jax.random.permutation(keys[0], FH)
    quick = order < FH // 2
    quick_rate = 1.0 / jax.random.uniform(keys[1], (FH,), jnp.float32, 30.0, 100.0)
    slow_rate = jax.random.uniform(keys[2], (FH,), jnp.float32, 0.5, 2.0) / TOKENS
    rates = jnp.where(quick, quick_rate, slow_rate)
    blocks = TOKENS // TOK_DEV
    factor = jnp.exp(jax.random.uniform(keys[3], (blocks, 1), jnp.float32, -0.7, 0.7))
    factor = jnp.repeat(factor, TOK_DEV, axis=0)
    jitter = jax.random.uniform(keys[4], (TOKENS, FH), jnp.float32, 0.3, 1.7)
    increments = -rates[None, :] * factor * jitter
    spots = jax.random.randint(keys[5], (3,), 0, TOKENS)
    struck = jnp.any(jnp.arange(TOKENS)[:, None] == spots[None, :], axis=1)
    losses = jax.random.uniform(keys[6], (TOKENS, FH), jnp.float32, 0.22, 0.69)
    increments = increments - jnp.where(struck[:, None], losses, 0.0)
    return jnp.cumsum(increments, axis=0)


def block_scale(own_key, extent, cuts, least, top_value):
    gain, own = 1.0, jax.random.fold_in(own_key, 6)
    for axis_at, blocks in cuts:
        heights = jnp.exp(jax.random.uniform(jax.random.fold_in(own, axis_at), (blocks,), jnp.float32, least / len(cuts), top_value / len(cuts)))
        gain = gain * jnp.repeat(heights, extent[axis_at] // blocks).reshape([-1 if axis == axis_at else 1 for axis in range(len(extent))])
    return gain


def noise(key, extent, scale, limit, cuts=(), held_as=jnp.bfloat16):
    gain = block_scale(key, extent, cuts, -0.22, 0.18) if cuts else 1.0
    entries = jax.random.normal(key, extent, jnp.float32) * scale * gain
    return jnp.minimum(jnp.maximum(entries, -limit), limit).astype(held_as)


def setup_inputs(seed: int = 0, part: int = 0) -> dict:
    key_list = jax.random.split(jax.random.key(seed), 15)
    own_keys = jax.random.split(jax.random.fold_in(key_list[14], part), 15)
    return {
        "tokens": noise(own_keys[0], (TOKENS, D), 1.0, 6.0, ((0, 64), (1, 4))),
        "norm_gain": jnp.clip(1.0 + 0.18 * jax.random.normal(key_list[1], (D,), jnp.float32), 0.1, 1.9),
        "ret_query_weight": noise(key_list[2], (D, RETAIN_HEADS * DK), D ** -0.5, 0.125, ((0, 64), (1, 4))),
        "ret_key_weight": noise(key_list[3], (D, RETAIN_HEADS * DK), D ** -0.5, 0.125, ((0, 64), (1, 4))),
        "ret_value_weight": noise(key_list[4], (D, RETAIN_HEADS * RETAIN_VALUE_DIM), D ** -0.5, 0.125, ((0, 64), (1, 4))),
        "fox_query_weight": draw_fox_query_weight(jax.random.fold_in(key_list[14], 71), part),
        "fox_key_weight": noise(key_list[6], (D, FH * FD), D ** -0.5, 0.125, ((0, 64), (1, 4))),
        "fox_value_weight": noise(key_list[7], (D, FH * FD), D ** -0.5, 0.125, ((0, 64), (1, 4))),
        "ret_decay": draw_ret_decay(jax.random.fold_in(key_list[14], 71), part),
        "ret_state": draw_ret_state(jax.random.fold_in(jax.random.fold_in(key_list[14], part), 71), part),
        "head_norm_gain": jnp.clip(1.0 + 0.18 * jax.random.normal(key_list[10], (RETAIN_HEADS * RETAIN_VALUE_DIM,), jnp.float32), 0.1, 1.9),
        "fox_gates": draw_fox_gates(jax.random.fold_in(jax.random.fold_in(key_list[14], part), 71), part),
        "ret_out_weight": noise(key_list[12], (RETAIN_HEADS * RETAIN_VALUE_DIM, D), (RETAIN_HEADS * RETAIN_VALUE_DIM + FH * FD) ** -0.5, 0.1875, ((0, 4), (1, 64))),
        "fox_out_weight": noise(key_list[13], (FH * FD, D), (FH * FD // 16) ** -0.5, 1.0, ((0, 4), (1, 64))),
    }


epsilon = 1e-06
highest = lax.Precision.HIGHEST

def head_group_norm(joined_output, norm_gains):
    center = joined_output - lax.optimization_barrier(jnp.mean(joined_output, axis=-1, keepdims=True))
    spread = lax.optimization_barrier(jnp.mean(center * center, axis=-1, keepdims=True))
    normal = center * lax.rsqrt(spread + epsilon) * norm_gains.reshape(joined_output.shape[1], joined_output.shape[2])
    return normal.reshape(joined_output.shape[0], -1).astype(jnp.bfloat16)

def retention(query_rows, key_rows, value_rows, log_decay, initial, norm_gains):
    sequence_length = query_rows.shape[0]
    blocks = sequence_length // TOK_DEV
    queries = query_rows.astype(jnp.float32).reshape(blocks, TOK_DEV, RETAIN_HEADS, DK)
    keys_all = key_rows.astype(jnp.float32).reshape(blocks, TOK_DEV, RETAIN_HEADS, DK) * DK ** (-0.5)
    values_all = value_rows.astype(jnp.float32).reshape(blocks, TOK_DEV, RETAIN_HEADS, RETAIN_VALUE_DIM)
    offsets = jnp.arange(TOK_DEV, dtype=jnp.float32)
    spread = offsets[:, None] - offsets[None, :]
    within = jnp.where(spread[None] >= 0, jnp.exp(jnp.maximum(spread, 0.0)[None] * log_decay[:, None, None]), 0.0)
    leading = jnp.exp((offsets + 1.0)[:, None] * log_decay[None, :])
    trailing = jnp.exp((TOK_DEV - 1.0 - offsets)[:, None] * log_decay[None, :])
    blockwise = jnp.exp(TOK_DEV * log_decay)

    def advance(memory, inputs):
        qblock, kblock, vblock = inputs
        scores = jnp.einsum('ihd,jhd->hij', qblock, kblock, precision=highest) * within
        inner_value = jnp.einsum('hij,jhe->ihe', scores, vblock, precision=highest)
        carried_state = jnp.einsum('ihd,hde->ihe', qblock, memory, precision=highest) * leading[:, :, None]
        summary = jnp.einsum('jhd,jhe->hde', kblock * trailing[:, :, None], vblock, precision=highest)
        return (memory * blockwise[:, None, None] + summary, inner_value + carried_state)
    _, output_rows = lax.scan(advance, initial, (queries, keys_all, values_all))
    return head_group_norm(output_rows.reshape(sequence_length, RETAIN_HEADS, RETAIN_VALUE_DIM), norm_gains)

def forgetting(query_rows, key_rows, value_rows, gates):
    sequence_length = query_rows.shape[0]
    queries = query_rows.astype(jnp.float32).reshape(sequence_length, FH, FD)
    keys_all = key_rows.astype(jnp.float32).reshape(sequence_length, FH, FD)
    values_all = value_rows.astype(jnp.float32).reshape(sequence_length, FH, FD)
    key_gates = gates.T
    key_pos = jnp.arange(sequence_length, dtype=jnp.int32)

    def block(number):
        first = (number * TOK_DEV).astype(jnp.int32)
        qblock = lax.dynamic_slice_in_dim(queries, first, TOK_DEV, 0)
        own_gates = lax.dynamic_slice_in_dim(key_gates, first, TOK_DEV, 1)
        scores = jnp.einsum('qhd,khd->hqk', qblock, keys_all) * FD ** (-0.5)
        scores = scores + own_gates[:, :, None] - key_gates[:, None, :]
        query_pos = first + jnp.arange(TOK_DEV, dtype=jnp.int32)
        scores = jnp.where(key_pos[None, None, :] <= query_pos[None, :, None], scores, -jnp.inf)
        highest_score = lax.optimization_barrier(jnp.max(scores, axis=-1, keepdims=True))
        weights = jnp.exp(scores - highest_score)
        totals = lax.optimization_barrier(jnp.sum(weights, axis=-1))
        rounded = lax.optimization_barrier(weights.astype(jnp.bfloat16)).astype(jnp.float32)
        weighted = jnp.einsum('hqk,khd->hqd', rounded, values_all)
        result = weighted / totals[:, :, None]
        return jnp.transpose(result, (1, 0, 2)).reshape(TOK_DEV, FH * FD).astype(jnp.bfloat16)
    pieces = lax.map(block, jnp.arange(sequence_length // TOK_DEV, dtype=jnp.int32))
    return pieces.reshape(sequence_length, FH * FD)

def reference(tokens, norm_gain, ret_query_weight, ret_key_weight, ret_value_weight, fox_query_weight, fox_key_weight, fox_value_weight, ret_decay, ret_state, head_norm_gain, fox_gates, ret_out_weight, fox_out_weight):
    widened = tokens.astype(jnp.float32)
    normed = (widened * lax.rsqrt(lax.optimization_barrier(jnp.mean(widened * widened, axis=-1, keepdims=True)) + epsilon) * norm_gain).astype(jnp.bfloat16)
    matrices = (ret_query_weight, ret_key_weight, ret_value_weight, fox_query_weight, fox_key_weight, fox_value_weight)
    ret_query, ret_key, ret_value, fox_query, fox_key, fox_value = [jnp.dot(normed, matrix, preferred_element_type=jnp.float32).astype(jnp.bfloat16) for matrix in matrices]
    retention_mixed = retention(ret_query, ret_key, ret_value, ret_decay, ret_state, head_norm_gain)
    fox_mix = forgetting(fox_query, fox_key, fox_value, fox_gates)
    ret_width = RETAIN_HEADS * RETAIN_VALUE_DIM // N_TP
    fox_width = FH * FD // N_TP
    summed = jnp.zeros((tokens.shape[0], D), jnp.float32)
    for member in range(N_TP):
        portion = jnp.dot(retention_mixed[:, member * ret_width:(member + 1) * ret_width], ret_out_weight[member * ret_width:(member + 1) * ret_width], preferred_element_type=jnp.float32)
        portion = portion + jnp.dot(fox_mix[:, member * fox_width:(member + 1) * fox_width], fox_out_weight[member * fox_width:(member + 1) * fox_width], preferred_element_type=jnp.float32)
        summed = summed + lax.optimization_barrier(portion.astype(jnp.bfloat16)).astype(jnp.float32)
    return summed.astype(jnp.bfloat16)
```

```python
import functools
import math

import jax
import jax.numpy as jnp
from jax import lax
from jax.experimental import pallas as pl
from jax.experimental.pallas import tpu as pltpu
from jax.sharding import PartitionSpec as P

MESH = pl.DeviceIdType.MESH
EPS = 1e-06
F32 = jnp.float32
BF16 = jnp.bfloat16
LOG2E = 1.4426950408889634
LOW = -3.0e38


def nt(a, b):
    return lax.dot_general(a, b, (((1,), (1,)), ((), ())), preferred_element_type=F32)


def nn(a, b):
    return jnp.dot(a, b, preferred_element_type=F32)


def split(a):
    high = a.astype(BF16)
    return high, (a - high.astype(F32)).astype(BF16)


def kernel(
    Z, X,
    tok, gain, rqw, rkw, rvw, fqw, fkw, fvw, dec, state, hng, gates, row, fow,
    out,
    wall, wsend, tokall, normed, kv, qbuf, rbuf, rin, summ, dall, mx, tot, acc, ot, mix, mixall,
    swap_s, swap_r, tok_s, tok_r, tokc_s, tokc_r, tok_l, ws, wr, ks, kr, ss, sr,
    ot_s, ot_r, otc_s, otc_r, ot_l, mix_s, mix_r,
):
    sp = lax.axis_index("sp")
    x = lax.axis_index("tp")
    c = lax.rem(sp, 2)
    z = sp // 2
    H = Z // 2
    rows_w = rqw.shape[0]
    chip_w = 2 * rows_w
    D = gain.shape[1]
    T, feat = tok.shape
    C = 2 * T
    Q = C // 4
    out_rows = T // X

    def at_z(k):
        return {"sp": lax.rem(z + k + Z, Z) * 2 + c}

    right, left = at_z(1), at_z(-1)
    sib = {"sp": z * 2 + 1 - c}
    peers = [{"tp": lax.rem(x + r, X)} for r in range(1, X)]
    cross = [{"tp": lax.rem(x + r, X), "sp": z * 2 + 1 - c} for r in range(1, X)]

    def remote(src, dst, s, r, dev):
        return pltpu.make_async_remote_copy(
            src_ref=src, dst_ref=dst, send_sem=s, recv_sem=r, device_id=dev, device_id_type=MESH
        )

    def head_block(h):
        def cut(ref, width):
            return ref[:, h * width : (h + 1) * width].astype(F32)

        half = rqw.shape[1] // 2
        wide = rvw.shape[1] // 2
        kvw = jnp.concatenate([cut(fkw, wide), cut(fvw, wide)], axis=1)
        rw = jnp.concatenate([cut(rvw, wide), cut(rqw, half), cut(rkw, half)], axis=1)
        fq = cut(fqw, wide)
        qw = jnp.concatenate([fq, jnp.zeros_like(fq)], axis=1)
        return kvw, rw, qw

    first, second = head_block(0), head_block(1)
    outs = jnp.concatenate(
        [row[...].astype(F32), fow[...].astype(F32), jnp.zeros((row.shape[0], 64), F32)], axis=1
    ).T
    ro, fo = outs[:rows_w], outs[rows_w : 2 * rows_w]
    wide = ro.shape[1] // 2
    out_first = jnp.concatenate([ro[:, :wide], fo[:, :wide]], axis=1)
    out_second = jnp.concatenate([ro[:, wide:], fo[:, wide:]], axis=1)
    is0 = c == 0
    own_rows = pl.ds(pl.multiple_of(z * chip_w + c * rows_w, rows_w), rows_w)
    blocks = [(first[0], second[0]), (first[1], second[1]), (out_first, out_second), (first[2], second[2])]
    for k, (a, b) in enumerate(blocks):
        wall[k, own_rows, :] = jnp.where(is0, a, b).astype(BF16)
        wsend[k] = jnp.where(is0, b, a).astype(BF16)

    barrier = pltpu.get_barrier_semaphore()
    partners = [right, left, sib] + peers + cross
    for dev in partners:
        pl.semaphore_signal(barrier, inc=1, device_id=dev, device_id_type=MESH)
    pl.semaphore_wait(barrier, len(partners))

    swap = remote(wsend, wall.at[:, own_rows, :], swap_s, swap_r, sib)
    swap.start()

    def tok_at(core, member):
        return tokall.at[core, :, pl.ds(pl.multiple_of(member * feat, feat), feat)]

    def source(r):
        return lax.rem(x - r + X, X)

    tok_sends = [remote(tok, tok_at(c, x), tok_s.at[r], tok_r.at[r], peers[r]) for r in range(X - 1)]
    for copy in tok_sends:
        copy.start()
    tok_cross = [remote(tok, tok_at(c, x), tokc_s.at[0], tokc_r.at[0], sib)]
    for r in range(1, X):
        tok_cross.append(
            remote(tok_at(c, source(r)), tok_at(c, source(r)), tokc_s.at[r], tokc_r.at[r], sib)
        )
    tok_cross[0].start()
    tok_own = pltpu.make_async_copy(tok, tok_at(c, x), tok_l)
    tok_own.start()

    gate_ref = jnp.where(is0, gates[0:1, pl.ds(pl.multiple_of(z * C, C), 128)], gates[1:2, pl.ds(pl.multiple_of(z * C, C), 128)])
    gate_row = jnp.where(is0, gates[0:1, :], gates[1:2, :])
    dall[...] = (gate_ref[:, 0:1] - gate_row) * LOG2E

    swap.wait()

    def ring_copy(buf_at, way, k, o, sems_s, sems_r, s):
        where = buf_at(k, o)
        return remote(where, where, sems_s.at[way, k], sems_r.at[way, s - 1, k], right if way == 0 else left)

    def origin(way, s):
        return lax.rem(z - s + Z, Z) if way == 0 else lax.rem(z + s, Z)

    def ring_start(buf_at, sems_s, sems_r, k):
        for way in range(2):
            ring_copy(buf_at, way, k, z, sems_s, sems_r, 1).start()

    def ring_step(buf_at, sems_s, sems_r, s, k):
        def one(way, mine):
            @pl.when(jnp.logical_or(s < H, mine))
            def _():
                o = origin(way, s)
                ring_copy(buf_at, way, k, o, sems_s, sems_r, s).wait_recv()

                @pl.when(jnp.logical_or(s + 1 < H, jnp.logical_and(s < H, mine)))
                def _():
                    nxt = ring_copy(buf_at, way, k, o, sems_s, sems_r, s + 1)
                    nxt.wait_send()
                    nxt.start()

        one(0, k < 2)
        one(1, k >= 2)

    def ring_end(buf_at, sems_s, sems_r, k):
        for way in range(2):
            ring_copy(buf_at, way, k, z, sems_s, sems_r, 1).wait_send()

    def wall_at(k, o):
        return wall.at[k, pl.ds(pl.multiple_of(o * chip_w, chip_w), chip_w), :]

    for k in range(4):
        ring_start(wall_at, ws, wr, k)

    pieces = 8
    stride = max(1, 4 * H // (2 * pieces))
    base = 4 * H - pieces * stride
    tok_step = base * 3 // 4
    P_rows = C // pieces

    def normalize(p):
        at = lax.rem(c * (pieces // 2) + p, pieces)
        half = at // (pieces // 2)
        lines = pl.ds(pl.multiple_of(lax.rem(at, pieces // 2) * P_rows, P_rows), P_rows)
        wide_rows = tokall[half, lines, :].astype(F32)
        scale = lax.rsqrt(jnp.mean(wide_rows * wide_rows, axis=1, keepdims=True) + EPS)
        normed[pl.ds(pl.multiple_of(at * P_rows, P_rows), P_rows), :] = (
            wide_rows * scale * gain[...]
        ).astype(BF16)

    def weights_loop(idx, carry):
        s = idx // 4 + 1
        k = lax.rem(idx, 4)
        ring_step(wall_at, ws, wr, s, k)

        @pl.when(idx == tok_step)
        def _():
            tok_own.wait()
            for r in range(1, X):
                tok_sends[r - 1].wait_recv()
                tok_cross[r].start()

        @pl.when(jnp.logical_and(idx >= base, lax.rem(idx - base, stride) == 0))
        def _():
            p = (idx - base) // stride

            @pl.when(p == pieces // 2)
            def _():
                for copy in tok_cross:
                    copy.wait_recv()

            normalize(p)

        return carry

    lax.fori_loop(0, 4 * H, weights_loop, 0)

    def project(k, dst, first_row):
        def body(i, carry):
            rows = pl.ds(pl.multiple_of(i * Q, Q), Q)
            dst[pl.ds(pl.multiple_of(first_row + i * Q, Q), Q), :] = nn(normed[rows, :], wall[k]).astype(BF16)
            return carry

        lax.fori_loop(0, 4, body, 0)

    def kv_at(k, o):
        return kv.at[pl.ds(pl.multiple_of(o * C + k * Q, Q), Q), :]

    def summ_at(k, o):
        return summ.at[o]

    project(0, kv, z * C)
    for k in range(3):
        ring_start(kv_at, ks, kr, k)
    project(3, qbuf, 0)
    ring_start(kv_at, ks, kr, 3)
    project(1, rbuf, 0)

    def ot_at(member, core):
        return ot.at[member, :, pl.ds(pl.multiple_of(core * 128, 128), 128)]

    ot_sends = [remote(wall.at[2], ot_at(x, c), ot_s.at[r], ot_r.at[r], peers[r]) for r in range(X - 1)]
    for copy in ot_sends:
        copy.start()
    ot_cross = [remote(wall.at[2], ot_at(x, c), otc_s.at[0], otc_r.at[0], sib)]
    for r in range(1, X):
        ot_cross.append(
            remote(ot_at(source(r), c), ot_at(source(r), c), otc_s.at[r], otc_r.at[r], sib)
        )
    ot_cross[0].start()
    ot_own = pltpu.make_async_copy(wall.at[2], ot_at(x, c), ot_l)
    ot_own.start()

    a = jnp.where(is0, dec[0], dec[1])
    key_size = rqw.shape[1] // 2
    key_scale = key_size ** (-0.5)
    lane = lax.broadcasted_iota(jnp.int32, (C, 128), 1)
    sub = lax.broadcasted_iota(jnp.int32, (C, 128), 0)
    trail = jnp.exp((C - 1.0 - sub.astype(F32)) * a) * key_scale
    turned = (rbuf[...].astype(F32) * trail).T
    t_high, t_low = split(turned)
    grown = nn(t_high, rbuf[...]) + nn(t_low, rbuf[...])
    lane16 = lax.broadcasted_iota(jnp.int32, (16, 128), 1)
    summ[z] = jnp.where(lane16 < 64, grown[96:112, :], pltpu.roll(grown[112:128, :], 64, 1))

    mx[...] = jnp.full_like(mx, LOW)
    tot[...] = jnp.zeros_like(tot)
    acc[...] = jnp.zeros_like(acc)
    fox_scale = (fqw.shape[1] // 2) ** (-0.5) * LOG2E

    def attend(i, j, masked):
        rows = pl.ds(pl.multiple_of(i * Q, Q), Q)
        block = kv[pl.ds(pl.multiple_of(j * C, C), C), :]
        s = nt(qbuf[rows, :], block) * fox_scale + dall[:, pl.ds(pl.multiple_of(j * C, C), C)]
        if masked:
            q_at = lax.broadcasted_iota(jnp.int32, s.shape, 0) + i * Q
            k_at = lax.broadcasted_iota(jnp.int32, s.shape, 1)
            s = jnp.where(k_at <= q_at, s, LOW)
        old = mx[rows, :]
        new = jnp.maximum(old, jnp.max(s, axis=1, keepdims=True))
        alpha = jnp.exp2(old - new)
        parts = [jnp.exp2(s[:, n * 128 : (n + 1) * 128] - new) for n in range(C // 128)]
        total = alpha * tot[rows, :]
        for part in parts:
            total = total + part
        tot[rows, :] = total
        mx[rows, :] = new
        weights = jnp.concatenate([part.astype(BF16) for part in parts], axis=1)
        acc[rows, :] = alpha * acc[rows, :] + nn(weights, block)

    def inner(i):
        rows = pl.ds(pl.multiple_of(i * Q, Q), Q)
        lanes = lax.broadcasted_iota(jnp.int32, (Q, 128), 1)
        query = jnp.where(jnp.logical_and(lanes >= 64, lanes < 96), rbuf[rows, :].astype(F32), 0.0).astype(BF16)
        keys = pltpu.roll(rbuf[...].astype(F32), 96, 1).astype(BF16)
        s = nt(query, keys)
        gap = lax.broadcasted_iota(jnp.int32, s.shape, 0) + i * Q - lax.broadcasted_iota(jnp.int32, s.shape, 1)
        within = jnp.where(gap >= 0, jnp.exp(jnp.maximum(gap, 0).astype(F32) * a), 0.0)
        high, low = split(s * key_scale * within)
        rin[rows, :] = nn(high, rbuf[...]) + nn(low, rbuf[...])

    def past(i, s):
        @pl.when(z - s >= 0)
        def _():
            attend(i, z - s, False)

        @pl.when(jnp.logical_and(z + s >= Z, s < H))
        def _():
            attend(i, z + s - Z, False)

    def attend_loop(idx, carry):
        s = idx // 4 + 1
        k = lax.rem(idx, 4)
        ring_step(kv_at, ks, kr, s, k)

        @pl.when(k == 3)
        def _():
            for way in range(2):
                @pl.when(jnp.logical_or(s < H, way == 0))
                def _(way=way):
                    o = origin(way, s)
                    ring_copy(summ_at, way, 0, o, ss, sr, s).wait_recv()

                    @pl.when(jnp.logical_or(s + 1 < H, jnp.logical_and(s < H, way == 0)))
                    def _():
                        nxt = ring_copy(summ_at, way, 0, o, ss, sr, s + 1)
                        nxt.wait_send()
                        nxt.start()

        @pl.when(s == 1)
        def _():
            inner(k)
            attend(k, z, True)

        @pl.when(s > 1)
        def _():
            past(k, s - 1)

        @pl.when(idx == 4 * H - 8)
        def _():
            for r in range(1, X):
                ot_sends[r - 1].wait_recv()
                ot_cross[r].start()

        return carry

    ring_start(summ_at, ss, sr, 0)
    lax.fori_loop(0, 4 * H, attend_loop, 0)

    def last(i, carry):
        past(i, H)
        return carry

    lax.fori_loop(0, 4, last, 0)

    span = float(C)
    far = z.astype(F32) * span

    def gather_state(j, total):
        gap = jnp.maximum(z - 1 - j, 0).astype(F32) * span
        weight = jnp.where(j < z, jnp.exp(jnp.zeros((16, 128), F32) + gap * a), 0.0)
        return total + weight * summ[j]

    packed = lax.fori_loop(0, Z, gather_state, jnp.zeros((16, 128), F32))
    both = jnp.concatenate([packed, pltpu.roll(packed, 64, 1)], axis=0)
    start = jnp.where(is0, state[0], state[1])
    start = jnp.concatenate([start, jnp.zeros_like(start)], axis=1)
    lane32 = lax.broadcasted_iota(jnp.int32, (32, 128), 1)
    entering = jnp.where(lane32 < 64, both, 0.0) + jnp.exp(jnp.zeros((32, 128), F32) + far * a) * start
    entering = jnp.concatenate([jnp.zeros((64, 128), F32), entering, jnp.zeros((32, 128), F32)], axis=0)
    e_high, e_low = split(entering)
    hn = hng[...]
    hn = jnp.where(is0, hn, pltpu.roll(hn, 64, 1))

    def finish(i, carry):
        rows = pl.ds(pl.multiple_of(i * Q, Q), Q)
        lanes = lax.broadcasted_iota(jnp.int32, (Q, 128), 1)
        place = (lax.broadcasted_iota(jnp.int32, (Q, 128), 0) + i * Q).astype(F32)
        leading = jnp.exp((place + 1.0) * a)
        query = rbuf[rows, :]
        raw = rin[rows, :] + (nn(query, e_high) + nn(query, e_low)) * leading
        raw = jnp.where(lanes < 64, raw, 0.0)
        center = jnp.where(lanes < 64, raw - jnp.sum(raw, axis=1, keepdims=True) * (1.0 / 64), 0.0)
        spread = jnp.sum(center * center, axis=1, keepdims=True) * (1.0 / 64)
        ret = center * lax.rsqrt(spread + EPS) * hn
        fox = acc[rows, :] / jnp.sum(tot[rows, :], axis=1, keepdims=True)
        mix[rows, :] = jnp.where(lanes < 64, ret, fox).astype(BF16)
        return carry

    lax.fori_loop(0, 4, finish, 0)

    def mix_rows(core, member):
        return mix.at[pl.ds(pl.multiple_of(core * T + member * out_rows, out_rows), out_rows), :]

    here = mixall.at[x, :, pl.ds(pl.multiple_of(c * 128, 128), 128)]
    mix_sends = [remote(mix_rows(1 - c, x), here, mix_s.at[0], mix_r.at[0], sib)]
    for r in range(1, X):
        member = lax.rem(x + r, X)
        mix_sends.append(remote(mix_rows(c, member), here, mix_s.at[2 * r - 1], mix_r.at[2 * r - 1], peers[r - 1]))
        mix_sends.append(remote(mix_rows(1 - c, member), here, mix_s.at[2 * r], mix_r.at[2 * r], cross[r - 1]))
    for copy in mix_sends:
        copy.start()
    mixall[x, :, pl.ds(pl.multiple_of(c * 128, 128), 128)] = mix[
        pl.ds(pl.multiple_of(c * T + x * out_rows, out_rows), out_rows), :
    ]
    ot_own.wait()
    for copy in ot_cross:
        copy.wait_recv()
    for copy in mix_sends:
        copy.wait_recv()

    tile = 256

    def project_out(n, carry):
        cols = pl.ds(pl.multiple_of(n * tile, tile), tile)
        total = jnp.zeros((out_rows, tile), F32)
        for g in range(X):
            total = total + nt(mixall[g], ot[g, cols, :]).astype(BF16).astype(F32)
        out[:, cols] = total.astype(BF16)
        return carry

    lax.fori_loop(0, D // tile, project_out, 0)

    for copy in tok_sends + tok_cross + ot_sends + ot_cross + mix_sends:
        copy.wait_send()
    for k in range(4):
        ring_end(wall_at, ws, wr, k)
        ring_end(kv_at, ks, kr, k)
    ring_end(summ_at, ss, sr, 0)


def local(Z, X, tokens, norm_gain, rqw, rkw, rvw, fqw, fkw, fvw, decay, state, hng, gates, row, fow):
    T = tokens.shape[0]
    C = 2 * T
    D = norm_gain.shape[0]
    H = Z // 2
    vm = pl.BlockSpec(memory_space=pltpu.VMEM)
    dma = pltpu.SemaphoreType.DMA
    in_specs = [vm] * 14
    in_specs[8] = pl.BlockSpec(memory_space=pltpu.SMEM)
    return pl.pallas_call(
        functools.partial(kernel, Z, X),
        out_shape=jax.ShapeDtypeStruct((T // X, D), BF16),
        in_specs=in_specs,
        out_specs=vm,
        scratch_shapes=[
            pltpu.VMEM((4, D, 128), BF16),
            pltpu.VMEM((4, rqw.shape[0], 128), BF16),
            pltpu.VMEM((2, T, D), BF16),
            pltpu.VMEM((C, D), BF16),
            pltpu.VMEM((Z * C, 128), BF16),
            pltpu.VMEM((C, 128), BF16),
            pltpu.VMEM((C, 128), BF16),
            pltpu.VMEM((C, 128), F32),
            pltpu.VMEM((Z, 16, 128), F32),
            pltpu.VMEM((1, Z * C), F32),
            pltpu.VMEM((C, 128), F32),
            pltpu.VMEM((C, 128), F32),
            pltpu.VMEM((C, 128), F32),
            pltpu.VMEM((X, D, 256), BF16),
            pltpu.VMEM((C, 128), BF16),
            pltpu.VMEM((X, T // X, 256), BF16),
            dma, dma,
            dma((X - 1,)), dma((X - 1,)), dma((X,)), dma((X,)), dma,
            dma((2, 4)), dma((2, H, 4)),
            dma((2, 4)), dma((2, H, 4)),
            dma((2, 1)), dma((2, H, 1)),
            dma((X - 1,)), dma((X - 1,)), dma((X,)), dma((X,)), dma,
            dma((2 * X - 1,)), dma((2 * X - 1,)),
        ],
        compiler_params=pltpu.CompilerParams(
            collective_id=0, has_side_effects=True, vmem_limit_bytes=56 * 1024 * 1024
        ),
    )(
        tokens, norm_gain.reshape(1, -1), rqw, rkw, rvw, fqw, fkw, fvw, decay, state,
        hng.reshape(1, -1), gates.T, row, fow,
    )


def solution(mesh):
    Z, X = mesh.shape["sp"] // 2, mesh.shape["tp"]
    return jax.shard_map(
        functools.partial(local, Z, X),
        mesh=mesh,
        in_specs=(
            P(("grp", "sp"), "tp"),
            P(),
            P("sp", "tp"),
            P("sp", "tp"),
            P("sp", "tp"),
            P("sp", "tp"),
            P("sp", "tp"),
            P("sp", "tp"),
            P("tp"),
            P(("grp", "tp"), None, None),
            P("tp"),
            P("grp", "tp"),
            P("tp", "sp"),
            P("tp", "sp"),
        ),
        out_specs=P(("grp", "sp", "tp"), None),
        check_vma=False,
    )
```

```python
import functools
import math

import jax
import jax.numpy as jnp
from jax import lax
from jax.experimental import pallas as pl
from jax.experimental.pallas import tpu as pltpu
from jax.sharding import PartitionSpec as P

MESH = pl.DeviceIdType.MESH
EPS = 1e-06
F32 = jnp.float32
BF16 = jnp.bfloat16
LOG2E = 1.4426950408889634
LOW = -3.0e38


def nt(a, b):
    return lax.dot_general(a, b, (((1,), (1,)), ((), ())), preferred_element_type=F32)


def nn(a, b):
    return jnp.dot(a, b, preferred_element_type=F32)


def split(a):
    high = a.astype(BF16)
    return high, (a - high.astype(F32)).astype(BF16)


def kernel(
    Z, X,
    tok, gain, rqw, rkw, rvw, fqw, fkw, fvw, dec, state, hng, gates, row, fow,
    out,
    wide_w, out_w, pack_w, query_w, send_w, send_o, send_p,
    tokall, normed, kv, qbuf, rbuf, rin, summ, dall, mx, tot, acc, ot, mix, mixall,
    swap_s, swap_r, tok_s, tok_r, tokc_s, tokc_r, tok_l, ws, wr, ks, kr, kl, ready,
    ot_s, ot_r, otc_s, otc_r, ot_l, mix_s, mix_r,
):
    sp = lax.axis_index("sp")
    x = lax.axis_index("tp")
    c = lax.rem(sp, 2)
    z = sp // 2
    H = Z // 2
    rows_w = rqw.shape[0]
    chip_w = 2 * rows_w
    D = gain.shape[1]
    T, feat = tok.shape
    C = 2 * T
    Q = C // 4
    out_rows = T // X
    is0 = c == 0

    def at_z(k):
        return {"sp": lax.rem(z + k + Z, Z) * 2 + c}

    hops = [(at_z(1), at_z(2)), (at_z(-1), at_z(-2))]
    sib = {"sp": z * 2 + 1 - c}
    final = {"sp": (Z - 1) * 2 + c}
    peers = [{"tp": lax.rem(x + r, X)} for r in range(1, X)]
    cross = [{"tp": lax.rem(x + r, X), "sp": z * 2 + 1 - c} for r in range(1, X)]

    def remote(src, dst, s, r, dev):
        return pltpu.make_async_remote_copy(
            src_ref=src, dst_ref=dst, send_sem=s, recv_sem=r, device_id=dev, device_id_type=MESH
        )

    def block(n, size):
        return pl.ds(pl.multiple_of(n * size, size), size)

    def head_block(h):
        def cut(ref):
            width = ref.shape[1] // 2
            return ref[:, h * width : (h + 1) * width].astype(F32)

        fq = cut(fqw)
        half = fq.shape[0] // 2
        return (
            jnp.concatenate([cut(fkw), cut(fvw), cut(rvw), cut(rqw), cut(rkw)], axis=1),
            jnp.concatenate([cut(row), cut(fow)], axis=1),
            jnp.concatenate([fq[:half], fq[half:]], axis=1),
        )

    first, second = head_block(0), head_block(1)
    own_rows = block(2 * z + c, rows_w)
    own_pack = block(2 * z + c, rows_w // 2)
    wide_w[own_rows, :] = jnp.where(is0, first[0], second[0]).astype(BF16)
    out_w[own_rows, :] = jnp.where(is0, first[1], second[1]).astype(BF16)
    pack_w[own_pack, :] = jnp.where(is0, first[2], second[2]).astype(BF16)
    send_w[...] = jnp.where(is0, second[0], first[0]).astype(BF16)
    send_o[...] = jnp.where(is0, second[1], first[1]).astype(BF16)
    send_p[...] = jnp.where(is0, second[2], first[2]).astype(BF16)

    barrier = pltpu.get_barrier_semaphore()
    partners = [hops[0][0], hops[0][1], hops[1][0], hops[1][1], sib] + peers + cross
    for dev in partners:
        pl.semaphore_signal(barrier, inc=1, device_id=dev, device_id_type=MESH)
    early = z <= H - 2
    is_last = z == Z - 1

    @pl.when(early)
    def _():
        pl.semaphore_signal(barrier, inc=1, device_id=final, device_id_type=MESH)

    pl.semaphore_wait(barrier, len(partners) + jnp.where(is_last, H - 1, 0))

    @pl.when(is_last)
    def _():
        for j in range(H - 1):
            pl.semaphore_signal(ready, inc=1, device_id={"sp": 2 * j + c}, device_id_type=MESH)

    swaps = [
        remote(send_w, wide_w.at[own_rows, :], swap_s.at[0], swap_r.at[0], sib),
        remote(send_o, out_w.at[own_rows, :], swap_s.at[1], swap_r.at[1], sib),
        remote(send_p, pack_w.at[own_pack, :], swap_s.at[2], swap_r.at[2], sib),
    ]
    for copy in swaps:
        copy.start()

    def source(r):
        return lax.rem(x - r + X, X)

    near = sorted({1, X - 1})

    def row_gather(src, at, s, r, cs, cr, local_sem):
        sends = [remote(src, at(x), s.at[n - 1], r.at[n - 1], peers[n - 1]) for n in near]
        over = [remote(src, at(x), cs.at[0], cr.at[0], sib)]
        over += [remote(at(source(n)), at(source(n)), cs.at[n], cr.at[n], sib) for n in near]
        own = pltpu.make_async_copy(src, at(x), local_sem)
        relays, later = [], []
        if X > 2:
            member = jnp.where(is0, source(1), source(X - 1))
            to = jnp.where(is0, lax.rem(x + 1, X), lax.rem(x + X - 1, X))
            relays = [remote(at(member), at(member), s.at[1], r.at[1], {"tp": to})]
            later = [remote(at(source(2)), at(source(2)), cs.at[2], cr.at[2], sib)]

        def begin():
            for copy in sends + over[:1]:
                copy.start()
            own.start()

        def middle():
            for copy in sends:
                copy.wait_recv()
            for copy in relays + over[1:]:
                copy.start()

        def close():
            own.wait()
            for copy in relays:
                copy.wait_recv()
            for copy in later:
                copy.start()

        def arrived():
            for copy in over + later:
                copy.wait_recv()

        def sent():
            for copy in sends + over + relays + later:
                copy.wait_send()

        return begin, middle, close, arrived, sent

    tok_all = row_gather(
        tok, lambda member: tokall.at[c, :, block(member, feat)], tok_s, tok_r, tokc_s, tokc_r, tok_l
    )
    tok_all[0]()

    nearby = gates[:, block(z, C)]
    gate_ref = jnp.where(is0, nearby[0:1, 0:128], nearby[1:2, 0:128])
    dall[...] = (gate_ref[:, 0:1] - jnp.where(is0, gates[0:1, :], gates[1:2, :])) * LOG2E

    for copy in swaps:
        copy.wait()

    def w_at(k, o):
        if k < 2:
            return wide_w.at[block(2 * o + k, rows_w), :]
        if k == 2:
            return out_w.at[block(o, chip_w), :]
        return pack_w.at[block(o, rows_w), :]

    def origin(way, d):
        return lax.rem(z - d + Z, Z) if way == 0 else lax.rem(z + d, Z)

    def w_copy(way, k, reach, o, t):
        return remote(
            w_at(k, o), w_at(k, o), ws.at[way, reach, k], wr.at[way, reach, t, k], hops[way][reach]
        )

    last_t = H // 2 - 1

    def w_step(t, k):
        for way in range(2):
            o = origin(way, 2 * t)

            @pl.when(t > 0)
            def _(way=way, o=o):
                w_copy(way, k, 1, o, t - 1).wait_recv()
                w_copy(way, k, 0, o, t).wait_send()

            w_copy(way, k, 0, o, t).start()
            mine = (k < 2) == (way == 0)

            def pass_two(way=way, o=o):
                @pl.when(t > 0)
                def _():
                    w_copy(way, k, 1, o, t).wait_send()

                w_copy(way, k, 1, o, t).start()

            if mine:
                pass_two()
            else:
                pl.when(t < last_t)(pass_two)

    pieces = 8
    P_rows = C // pieces
    rounds = last_t + 1
    w_total = 4 * rounds
    base = w_total // 2 + 1
    stride = 2
    inside = min(pieces, (w_total - base + stride - 1) // stride)

    def normalize(p):
        @pl.when(p == pieces // 2)
        def _():
            tok_all[3]()

        at = lax.rem(c * (pieces // 2) + p, pieces)
        half = at // (pieces // 2)
        values = tokall[half, block(lax.rem(at, pieces // 2), P_rows), :].astype(F32)
        scale = lax.rsqrt(jnp.mean(values * values, axis=1, keepdims=True) + EPS)
        normed[block(at, P_rows), :] = (values * scale * gain[...]).astype(BF16)

    def weights_loop(t, carry):
        for k in range(4):
            w_step(t, k)
            idx = 4 * t + k

            @pl.when(idx == w_total // 4)
            def _():
                tok_all[1]()

            @pl.when(idx == w_total // 2)
            def _():
                tok_all[2]()

            if k % 2 == 1:

                @pl.when(jnp.logical_and(idx >= base, idx < base + stride * inside))
                def _():
                    normalize((idx - base) // stride)

        return carry

    lax.fori_loop(0, rounds, weights_loop, 0)
    for p in range(inside, pieces):
        normalize(jnp.int32(p))

    def weights_end(t, carry):
        for k in range(4):
            for way in range(2):
                w_copy(way, k, 0, origin(way, 2 * t + 1), t).wait_recv()
        return carry

    lax.fori_loop(0, rounds, weights_end, 0)
    for k in range(4):
        way = 0 if k < 2 else 1
        w_copy(way, k, 1, origin(way, H), last_t).wait_recv()

    def project_wide(i, carry):
        rows = block(i, Q)
        both = nn(normed[rows, :], wide_w[...]).astype(BF16)
        kv[block(z * 4 + i, Q), :] = both[:, :128]
        rbuf[rows, :] = both[:, 128:]
        return carry

    lax.fori_loop(0, 4, project_wide, 0)

    def kv_at(k, o):
        return kv.at[block(o * 4 + k, Q), :] if k < 4 else summ.at[o]

    def right_copy(k, o, s):
        return remote(kv_at(k, o), kv_at(k, o), ks.at[0, k], kr.at[s - 1, k], hops[0][0])

    def left_copy(k, j, dev):
        return remote(kv_at(k, j), kv_at(k, j), ks.at[1, k], kl.at[j, k], dev)

    def kv_start(k):
        @pl.when(z < Z - 1)
        def _():
            right_copy(k, z, 1).start()

        @pl.when(early)
        def _():
            left_copy(k, jnp.minimum(z, H - 2), final).start()

    def left_block(s):
        return s - 2 - (Z - 1 - z)

    def kv_step(k, s):
        @pl.when(z - s >= 0)
        def _():
            o = z - s
            right_copy(k, o, s).wait_recv()

            @pl.when(jnp.logical_and(z < Z - 1, s < H))
            def _():
                nxt = right_copy(k, o, s + 1)
                nxt.wait_send()
                nxt.start()

        j = left_block(s)

        @pl.when(j >= 0)
        def _():
            copy = left_copy(k, j, hops[1][0])
            copy.wait_recv()

            @pl.when(j <= z - H - 2)
            def _():
                @pl.when(j >= 1)
                def _():
                    copy.wait_send()

                copy.start()

    def kv_end(k):
        @pl.when(z < Z - 1)
        def _():
            right_copy(k, z, 1).wait_send()

        @pl.when(jnp.logical_or(early, z >= H + 2))
        def _():
            left_copy(k, 0, final).wait_send()

    @pl.when(early)
    def _():
        pl.semaphore_wait(ready, 1)

    for k in range(4):
        kv_start(k)

    ot_all = row_gather(
        out_w, lambda member: ot.at[member, :, block(c, 128)], ot_s, ot_r, otc_s, otc_r, ot_l
    )
    ot_all[0]()

    lane_p = lax.broadcasted_iota(jnp.int32, (rows_w, 128), 1) < 64
    half_w = rows_w // 2

    def unpack(o, carry):
        packed = pack_w[block(o, rows_w), :].astype(F32)
        low = jnp.where(lane_p, packed, 0.0)
        high = jnp.where(lane_p, pltpu.roll(packed, 64, 1), 0.0)
        query_w[block(o, chip_w), :] = jnp.concatenate(
            [low[:half_w], high[:half_w], low[half_w:], high[half_w:]], axis=0
        ).astype(BF16)
        return carry

    lax.fori_loop(0, Z, unpack, 0, unroll=4)

    def project_query(i, carry):
        rows = block(i, Q)
        qbuf[rows, :] = nn(normed[rows, :], query_w[...]).astype(BF16)
        return carry

    lax.fori_loop(0, 4, project_query, 0)

    a = jnp.where(is0, dec[0], dec[1])
    key_size = rqw.shape[1] // 2
    key_scale = key_size ** (-0.5)
    sub = lax.broadcasted_iota(jnp.int32, (C, 128), 0)
    trail = jnp.exp((C - 1.0 - sub.astype(F32)) * a) * key_scale
    turned = (rbuf[...].astype(F32) * trail).T
    t_high, t_low = split(turned)
    grown = nn(t_high, rbuf[...]) + nn(t_low, rbuf[...])
    lane16 = lax.broadcasted_iota(jnp.int32, (16, 128), 1)
    summ[z] = jnp.where(lane16 < 64, grown[96:112, :], pltpu.roll(grown[112:128, :], 64, 1))

    mx[...] = jnp.full_like(mx, LOW)
    tot[...] = jnp.zeros_like(tot)
    acc[...] = jnp.zeros_like(acc)
    fox_scale = (fqw.shape[1] // 2) ** (-0.5) * LOG2E
    R = C // 2

    def attend(i, js, masked):
        rows = block(i, R)
        query = qbuf[rows, :]
        blocks = [kv[block(j, C), :] for j in js]
        scores = [nt(query, b) * fox_scale + dall[:, block(j, C)] for j, b in zip(js, blocks)]
        if masked:
            q_at = lax.broadcasted_iota(jnp.int32, (R, C), 0) + i * R
            k_at = lax.broadcasted_iota(jnp.int32, (R, C), 1)
            scores = [jnp.where(k_at <= q_at, s, LOW) for s in scores]
        tops = [s[:, n * 128 : (n + 1) * 128] for s in scores for n in range(C // 128)]
        top = functools.reduce(jnp.maximum, tops)
        old = mx[rows, :]
        new = jnp.maximum(old, jnp.max(top, axis=1, keepdims=True))
        alpha = jnp.exp2(old - new)
        parts = [jnp.exp2(s - new) for s in tops]
        tot[rows, :] = alpha * tot[rows, :] + functools.reduce(jnp.add, parts)
        mx[rows, :] = new
        each = C // 128
        weighted = [
            nn(jnp.concatenate([p.astype(BF16) for p in parts[n * each : (n + 1) * each]], axis=1), b)
            for n, b in enumerate(blocks)
        ]
        acc[rows, :] = alpha * acc[rows, :] + functools.reduce(jnp.add, weighted)

    def inner(i):
        rows = block(i, Q)
        lanes = lax.broadcasted_iota(jnp.int32, (Q, 128), 1)
        query = jnp.where(jnp.logical_and(lanes >= 64, lanes < 96), rbuf[rows, :].astype(F32), 0.0).astype(BF16)
        keys = pltpu.roll(rbuf[...].astype(F32), 96, 1).astype(BF16)
        s = nt(query, keys)
        gap = lax.broadcasted_iota(jnp.int32, s.shape, 0) + i * Q - lax.broadcasted_iota(jnp.int32, s.shape, 1)
        within = jnp.where(gap >= 0, jnp.exp(jnp.maximum(gap, 0).astype(F32) * a), 0.0)
        high, low = split(s * key_scale * within)
        rin[rows, :] = nn(high, rbuf[...]) + nn(low, rbuf[...])

    def past(i, s):
        j = left_block(s)

        @pl.when(jnp.logical_and(z - s >= 0, j < 0))
        def _():
            attend(i, [z - s], False)

        @pl.when(j >= 0)
        def _():
            attend(i, [z - s, j], False)

    def attend_loop(s, carry):
        for k in range(4):
            kv_step(k, s)
            if k == 3:
                kv_step(4, s)
            idx = 4 * (s - 1) + k

            @pl.when(s == 1)
            def _():
                inner(k)

            if k % 2 == 1:
                @pl.when(s == 1)
                def _():
                    attend(k // 2, [z], True)

                @pl.when(s > 1)
                def _():
                    past(k // 2, s - 1)

            if k == 0:
                @pl.when(idx == H)
                def _():
                    ot_all[1]()

                @pl.when(idx == max(H, 2 * H - 4))
                def _():
                    ot_all[2]()

        return carry

    kv_start(4)
    lax.fori_loop(1, H + 1, attend_loop, 0)

    def last(i, carry):
        past(i, H)
        return carry

    lax.fori_loop(0, 2, last, 0)

    span = float(C)
    far = z.astype(F32) * span

    def gather_state(j, total):
        gap = (z - 1 - j).astype(F32) * span
        return total + jnp.exp(jnp.zeros((16, 128), F32) + gap * a) * summ[j]

    packed = lax.fori_loop(0, z, gather_state, jnp.zeros((16, 128), F32))
    both = jnp.concatenate([packed, pltpu.roll(packed, 64, 1)], axis=0)
    start = jnp.where(is0, state[0], state[1])
    start = jnp.concatenate([start, jnp.zeros_like(start)], axis=1)
    lane32 = lax.broadcasted_iota(jnp.int32, (32, 128), 1)
    entering = jnp.where(lane32 < 64, both, 0.0) + jnp.exp(jnp.zeros((32, 128), F32) + far * a) * start
    entering = jnp.concatenate([jnp.zeros((64, 128), F32), entering, jnp.zeros((32, 128), F32)], axis=0)
    e_high, e_low = split(entering)
    hn = hng[...]
    hn = jnp.where(is0, hn, pltpu.roll(hn, 64, 1))

    def finish(i, carry):
        rows = pl.ds(pl.multiple_of(i * Q, Q), Q)
        lanes = lax.broadcasted_iota(jnp.int32, (Q, 128), 1)
        place = (lax.broadcasted_iota(jnp.int32, (Q, 128), 0) + i * Q).astype(F32)
        leading = jnp.exp((place + 1.0) * a)
        query = rbuf[rows, :]
        raw = rin[rows, :] + (nn(query, e_high) + nn(query, e_low)) * leading
        raw = jnp.where(lanes < 64, raw, 0.0)
        center = jnp.where(lanes < 64, raw - jnp.sum(raw, axis=1, keepdims=True) * (1.0 / 64), 0.0)
        spread = jnp.sum(center * center, axis=1, keepdims=True) * (1.0 / 64)
        ret = center * lax.rsqrt(spread + EPS) * hn
        fox = acc[rows, :] / jnp.sum(tot[rows, :], axis=1, keepdims=True)
        mix[rows, :] = jnp.where(lanes < 64, ret, fox).astype(BF16)
        return carry

    lax.fori_loop(0, 4, finish, 0)

    def mix_rows(core, member):
        return mix.at[pl.ds(pl.multiple_of(core * T + member * out_rows, out_rows), out_rows), :]

    here = mixall.at[x, :, pl.ds(pl.multiple_of(c * 128, 128), 128)]
    mix_sends = [remote(mix_rows(1 - c, x), here, mix_s.at[0], mix_r.at[0], sib)]
    for r in range(1, X):
        member = lax.rem(x + r, X)
        mix_sends.append(remote(mix_rows(c, member), here, mix_s.at[2 * r - 1], mix_r.at[2 * r - 1], peers[r - 1]))
        mix_sends.append(remote(mix_rows(1 - c, member), here, mix_s.at[2 * r], mix_r.at[2 * r], cross[r - 1]))
    for copy in mix_sends:
        copy.start()
    mixall[x, :, pl.ds(pl.multiple_of(c * 128, 128), 128)] = mix[
        pl.ds(pl.multiple_of(c * T + x * out_rows, out_rows), out_rows), :
    ]
    ot_all[3]()
    for copy in mix_sends:
        copy.wait_recv()

    tile = 256

    def project_out(n, carry):
        cols = pl.ds(pl.multiple_of(n * tile, tile), tile)
        total = jnp.zeros((out_rows, tile), F32)
        for g in range(X):
            total = total + nt(mixall[g], ot[g, cols, :]).astype(BF16).astype(F32)
        out[:, cols] = total.astype(BF16)
        return carry

    lax.fori_loop(0, D // tile, project_out, 0)

    for copy in mix_sends:
        copy.wait_send()
    tok_all[4]()
    ot_all[4]()
    for way in range(2):
        for reach in range(2):
            for k in range(4):
                w_copy(way, k, reach, z, 0).wait_send()
    for k in range(5):
        kv_end(k)


def local(Z, X, tokens, norm_gain, rqw, rkw, rvw, fqw, fkw, fvw, decay, state, hng, gates, row, fow):
    T = tokens.shape[0]
    C = 2 * T
    D = norm_gain.shape[0]
    H = Z // 2
    vm = pl.BlockSpec(memory_space=pltpu.VMEM)
    dma = pltpu.SemaphoreType.DMA
    in_specs = [vm] * 14
    in_specs[8] = pl.BlockSpec(memory_space=pltpu.SMEM)
    return pl.pallas_call(
        functools.partial(kernel, Z, X),
        out_shape=jax.ShapeDtypeStruct((T // X, D), BF16),
        in_specs=in_specs,
        out_specs=vm,
        scratch_shapes=[
            pltpu.VMEM((D, 256), BF16),
            pltpu.VMEM((D, 128), BF16),
            pltpu.VMEM((D // 2, 128), BF16),
            pltpu.VMEM((D, 128), BF16),
            pltpu.VMEM((rqw.shape[0], 256), BF16),
            pltpu.VMEM((rqw.shape[0], 128), BF16),
            pltpu.VMEM((rqw.shape[0] // 2, 128), BF16),
            pltpu.VMEM((2, T, D), BF16),
            pltpu.VMEM((C, D), BF16),
            pltpu.VMEM((Z * C, 128), BF16),
            pltpu.VMEM((C, 128), BF16),
            pltpu.VMEM((C, 128), BF16),
            pltpu.VMEM((C, 128), F32),
            pltpu.VMEM((Z, 16, 128), F32),
            pltpu.VMEM((1, Z * C), F32),
            pltpu.VMEM((C, 128), F32),
            pltpu.VMEM((C, 128), F32),
            pltpu.VMEM((C, 128), F32),
            pltpu.VMEM((X, D, 256), BF16),
            pltpu.VMEM((C, 128), BF16),
            pltpu.VMEM((X, T // X, 256), BF16),
            dma((3,)), dma((3,)),
            dma((X - 1,)), dma((X - 1,)), dma((X,)), dma((X,)), dma,
            dma((2, 2, 4)), dma((2, 2, H // 2, 4)),
            dma((2, 5)), dma((H, 5)), dma((H - 1, 5)), pltpu.SemaphoreType.REGULAR,
            dma((X - 1,)), dma((X - 1,)), dma((X,)), dma((X,)), dma,
            dma((2 * X - 1,)), dma((2 * X - 1,)),
        ],
        compiler_params=pltpu.CompilerParams(
            collective_id=0, has_side_effects=True, vmem_limit_bytes=56 * 1024 * 1024
        ),
    )(
        tokens, norm_gain.reshape(1, -1), rqw, rkw, rvw, fqw, fkw, fvw, decay, state,
        hng.reshape(1, -1), gates.T, row.T, fow.T,
    )


def solution(mesh):
    Z, X = mesh.shape["sp"] // 2, mesh.shape["tp"]
    return jax.shard_map(
        functools.partial(local, Z, X),
        mesh=mesh,
        in_specs=(
            P(("grp", "sp"), "tp"),
            P(),
            P("sp", "tp"),
            P("sp", "tp"),
            P("sp", "tp"),
            P("sp", "tp"),
            P("sp", "tp"),
            P("sp", "tp"),
            P("tp"),
            P(("grp", "tp"), None, None),
            P("tp"),
            P("grp", "tp"),
            P("tp", "sp"),
            P("tp", "sp"),
        ),
        out_specs=P(("grp", "sp", "tp"), None),
        check_vma=False,
    )
```

```python
import functools
import math

import jax
import jax.numpy as jnp
from jax import lax
from jax.experimental import pallas as pl
from jax.experimental.pallas import tpu as pltpu
from jax.sharding import PartitionSpec as P

MESH = pl.DeviceIdType.MESH
EPS = 1e-06
F32 = jnp.float32
BF16 = jnp.bfloat16
LOG2E = 1.4426950408889634
LOW = -3.0e38


def nt(a, b):
    return lax.dot_general(a, b, (((1,), (1,)), ((), ())), preferred_element_type=F32)


def nn(a, b):
    return jnp.dot(a, b, preferred_element_type=F32)


def split(a):
    high = a.astype(BF16)
    return high, (a - high.astype(F32)).astype(BF16)


def kernel(
    Z, X,
    tok, gain, rqw, rkw, rvw, fqw, fkw, fvw, dec, state, hng, gates, row, fow,
    out,
    wide_w, out_w, pack_w, query_w, send_w, send_o, send_p,
    tokall, normed, kv, qbuf, rbuf, rin, summ, dall, mx, tot, acc, ot, mix, mixall,
    swap_s, swap_r, tok_s, tok_r, tokc_s, tokc_r, tok_l, ws, wr, ks, kr, kl, ready,
    ot_s, ot_r, otc_s, otc_r, ot_l, mix_s, mix_r,
):
    sp = lax.axis_index("sp")
    x = lax.axis_index("tp")
    c = lax.rem(sp, 2)
    z = sp // 2
    H = Z // 2
    rows_w = rqw.shape[0]
    chip_w = 2 * rows_w
    D = gain.shape[1]
    T, feat = tok.shape
    C = 2 * T
    Q = C // 4
    out_rows = T // X
    is0 = c == 0

    def at_z(k):
        return {"sp": lax.rem(z + k + Z, Z) * 2 + c}

    hops = [(at_z(1), at_z(2)), (at_z(-1), at_z(-2))]
    sib = {"sp": z * 2 + 1 - c}
    final = {"sp": (Z - 1) * 2 + c}
    peers = [{"tp": lax.rem(x + r, X)} for r in range(1, X)]
    cross = [{"tp": lax.rem(x + r, X), "sp": z * 2 + 1 - c} for r in range(1, X)]

    def remote(src, dst, s, r, dev):
        return pltpu.make_async_remote_copy(
            src_ref=src, dst_ref=dst, send_sem=s, recv_sem=r, device_id=dev, device_id_type=MESH
        )

    def block(n, size):
        return pl.ds(pl.multiple_of(n * size, size), size)

    def head_block(h):
        def cut(ref):
            width = ref.shape[1] // 2
            return ref[:, h * width : (h + 1) * width].astype(F32)

        fq = cut(fqw)
        half = fq.shape[0] // 2
        return (
            jnp.concatenate([cut(fkw), cut(fvw), cut(rvw), cut(rqw), cut(rkw)], axis=1),
            jnp.concatenate([cut(row), cut(fow)], axis=1),
            jnp.concatenate([fq[:half], fq[half:]], axis=1),
        )

    first, second = head_block(0), head_block(1)
    own_rows = block(2 * z + c, rows_w)
    own_pack = block(2 * z + c, rows_w // 2)
    wide_w[own_rows, :] = jnp.where(is0, first[0], second[0]).astype(BF16)
    out_w[own_rows, :] = jnp.where(is0, first[1], second[1]).astype(BF16)
    pack_w[own_pack, :] = jnp.where(is0, first[2], second[2]).astype(BF16)
    send_w[...] = jnp.where(is0, second[0], first[0]).astype(BF16)
    send_o[...] = jnp.where(is0, second[1], first[1]).astype(BF16)
    send_p[...] = jnp.where(is0, second[2], first[2]).astype(BF16)

    barrier = pltpu.get_barrier_semaphore()
    partners = [hops[0][0], hops[0][1], hops[1][0], hops[1][1], sib] + peers + cross
    for dev in partners:
        pl.semaphore_signal(barrier, inc=1, device_id=dev, device_id_type=MESH)
    early = z <= H - 2
    is_last = z == Z - 1

    @pl.when(early)
    def _():
        pl.semaphore_signal(barrier, inc=1, device_id=final, device_id_type=MESH)

    pl.semaphore_wait(barrier, len(partners) + jnp.where(is_last, H - 1, 0))

    @pl.when(is_last)
    def _():
        for j in range(H - 1):
            pl.semaphore_signal(ready, inc=1, device_id={"sp": 2 * j + c}, device_id_type=MESH)

    swaps = [
        remote(send_w, wide_w.at[own_rows, :], swap_s.at[0], swap_r.at[0], sib),
        remote(send_o, out_w.at[own_rows, :], swap_s.at[1], swap_r.at[1], sib),
        remote(send_p, pack_w.at[own_pack, :], swap_s.at[2], swap_r.at[2], sib),
    ]
    for copy in swaps:
        copy.start()

    def source(r):
        return lax.rem(x - r + X, X)

    near = sorted({1, X - 1})

    def row_gather(src, at, s, r, cs, cr, local_sem):
        sends = [remote(src, at(x), s.at[n - 1], r.at[n - 1], peers[n - 1]) for n in near]
        over = [remote(src, at(x), cs.at[0], cr.at[0], sib)]
        over += [remote(at(source(n)), at(source(n)), cs.at[n], cr.at[n], sib) for n in near]
        own = pltpu.make_async_copy(src, at(x), local_sem)
        relays, later = [], []
        if X > 2:
            member = jnp.where(is0, source(1), source(X - 1))
            to = jnp.where(is0, lax.rem(x + 1, X), lax.rem(x + X - 1, X))
            relays = [remote(at(member), at(member), s.at[1], r.at[1], {"tp": to})]
            later = [remote(at(source(2)), at(source(2)), cs.at[2], cr.at[2], sib)]

        def begin():
            for copy in sends + over[:1]:
                copy.start()
            own.start()

        def middle():
            for copy in sends:
                copy.wait_recv()
            for copy in relays + over[1:]:
                copy.start()

        def close():
            own.wait()
            for copy in relays:
                copy.wait_recv()
            for copy in later:
                copy.start()

        def arrived():
            for copy in over + later:
                copy.wait_recv()

        def sent():
            for copy in sends + over + relays + later:
                copy.wait_send()

        return begin, middle, close, arrived, sent

    tok_all = row_gather(
        tok, lambda member: tokall.at[c, :, block(member, feat)], tok_s, tok_r, tokc_s, tokc_r, tok_l
    )
    tok_all[0]()

    nearby = gates[:, block(z, C)]
    gate_ref = jnp.where(is0, nearby[0:1, 0:128], nearby[1:2, 0:128])
    dall[...] = (gate_ref[:, 0:1] - jnp.where(is0, gates[0:1, :], gates[1:2, :])) * LOG2E

    for copy in swaps:
        copy.wait()

    def w_at(k, o):
        if k < 2:
            return wide_w.at[block(2 * o + k, rows_w), :]
        if k == 2:
            return out_w.at[block(o, chip_w), :]
        return pack_w.at[block(o, rows_w), :]

    def origin(way, d):
        return lax.rem(z - d + Z, Z) if way == 0 else lax.rem(z + d, Z)

    def w_copy(way, k, reach, o, t):
        return remote(
            w_at(k, o), w_at(k, o), ws.at[way, reach, k], wr.at[way, reach, t, k], hops[way][reach]
        )

    last_t = H // 2 - 1

    def w_step(t, k):
        for way in range(2):
            o = origin(way, 2 * t)

            @pl.when(t > 0)
            def _(way=way, o=o):
                w_copy(way, k, 1, o, t - 1).wait_recv()
                w_copy(way, k, 0, o, t).wait_send()

            w_copy(way, k, 0, o, t).start()
            mine = (k < 2) == (way == 0)

            def pass_two(way=way, o=o):
                @pl.when(t > 0)
                def _():
                    w_copy(way, k, 1, o, t).wait_send()

                w_copy(way, k, 1, o, t).start()

            if mine:
                pass_two()
            else:
                pl.when(t < last_t)(pass_two)

    pieces = 8
    P_rows = C // pieces
    rounds = last_t + 1
    w_total = 4 * rounds
    base = w_total // 2 + 1
    stride = 2
    inside = min(pieces, (w_total - base + stride - 1) // stride)

    def normalize(p):
        @pl.when(p == pieces // 2)
        def _():
            tok_all[3]()

        at = lax.rem(c * (pieces // 2) + p, pieces)
        half = at // (pieces // 2)
        values = tokall[half, block(lax.rem(at, pieces // 2), P_rows), :].astype(F32)
        scale = lax.rsqrt(jnp.mean(values * values, axis=1, keepdims=True) + EPS)
        normed[block(at, P_rows), :] = (values * scale * gain[...]).astype(BF16)

    def weights_loop(t, carry):
        for k in range(4):
            w_step(t, k)
            idx = 4 * t + k

            @pl.when(idx == w_total // 4)
            def _():
                tok_all[1]()

            @pl.when(idx == w_total // 2)
            def _():
                tok_all[2]()

            if k % 2 == 1:

                @pl.when(jnp.logical_and(idx >= base, idx < base + stride * inside))
                def _():
                    normalize((idx - base) // stride)

        return carry

    lax.fori_loop(0, rounds, weights_loop, 0)
    for p in range(inside, pieces):
        normalize(jnp.int32(p))

    def weights_end(t, carry):
        for k in range(4):
            for way in range(2):
                w_copy(way, k, 0, origin(way, 2 * t + 1), t).wait_recv()
        return carry

    lax.fori_loop(0, rounds, weights_end, 0)
    for k in range(4):
        way = 0 if k < 2 else 1
        w_copy(way, k, 1, origin(way, H), last_t).wait_recv()

    ot_all = row_gather(
        out_w, lambda member: ot.at[member, :, block(c, 128)], ot_s, ot_r, otc_s, otc_r, ot_l
    )
    ot_all[0]()

    def project_wide(i, carry):
        rows = block(i, Q)
        both = nn(normed[rows, :], wide_w[...]).astype(BF16)
        kv[block(z * 4 + i, Q), :] = both[:, :128]
        rbuf[rows, :] = both[:, 128:]
        return carry

    lax.fori_loop(0, 4, project_wide, 0)

    def kv_at(k, o):
        return kv.at[block(o * 4 + k, Q), :] if k < 4 else summ.at[o]

    def right_copy(k, o, s):
        return remote(kv_at(k, o), kv_at(k, o), ks.at[0, k], kr.at[s - 1, k], hops[0][0])

    def left_copy(k, j, dev):
        return remote(kv_at(k, j), kv_at(k, j), ks.at[1, k], kl.at[j, k], dev)

    def kv_start(k):
        @pl.when(z < Z - 1)
        def _():
            right_copy(k, z, 1).start()

    def left_block(s):
        return s - 2 - (Z - 1 - z)

    def kv_step(k, s):
        @pl.when(z - s >= 0)
        def _():
            o = z - s
            right_copy(k, o, s).wait_recv()

            @pl.when(jnp.logical_and(z < Z - 1, s < H))
            def _():
                nxt = right_copy(k, o, s + 1)
                nxt.wait_send()
                nxt.start()

        j = left_block(s)

        @pl.when(j >= 0)
        def _():
            copy = left_copy(k, j, hops[1][0])
            copy.wait_recv()

            @pl.when(j <= z - H - 2)
            def _():
                @pl.when(j >= 1)
                def _():
                    copy.wait_send()

                copy.start()

    def kv_end(k):
        @pl.when(z < Z - 1)
        def _():
            right_copy(k, z, 1).wait_send()

        @pl.when(jnp.logical_or(early, z >= H + 2))
        def _():
            left_copy(k, 0, final).wait_send()

    for k in range(4):
        kv_start(k)

    lane_p = lax.broadcasted_iota(jnp.int32, (rows_w, 128), 1) < 64
    half_w = rows_w // 2

    def unpack(o, carry):
        packed = pack_w[block(o, rows_w), :].astype(F32)
        low = jnp.where(lane_p, packed, 0.0)
        high = jnp.where(lane_p, pltpu.roll(packed, 64, 1), 0.0)
        query_w[block(o, chip_w), :] = jnp.concatenate(
            [low[:half_w], high[:half_w], low[half_w:], high[half_w:]], axis=0
        ).astype(BF16)
        return carry

    lax.fori_loop(0, Z, unpack, 0, unroll=4)

    def project_query(i, carry):
        rows = block(i, Q)
        qbuf[rows, :] = nn(normed[rows, :], query_w[...]).astype(BF16)
        return carry

    lax.fori_loop(0, 4, project_query, 0)

    a = jnp.where(is0, dec[0], dec[1])
    key_size = rqw.shape[1] // 2
    key_scale = key_size ** (-0.5)
    sub = lax.broadcasted_iota(jnp.int32, (C, 128), 0)
    trail = jnp.exp((C - 1.0 - sub.astype(F32)) * a) * key_scale
    turned = (rbuf[...].astype(F32) * trail).T
    t_high, t_low = split(turned)
    grown = nn(t_high, rbuf[...]) + nn(t_low, rbuf[...])
    lane16 = lax.broadcasted_iota(jnp.int32, (16, 128), 1)
    summ[z] = jnp.where(lane16 < 64, grown[96:112, :], pltpu.roll(grown[112:128, :], 64, 1))

    mx[...] = jnp.full_like(mx, LOW)
    tot[...] = jnp.zeros_like(tot)
    acc[...] = jnp.zeros_like(acc)
    fox_scale = (fqw.shape[1] // 2) ** (-0.5) * LOG2E
    R = C // 2

    def attend(i, js, masked):
        rows = block(i, R)
        query = qbuf[rows, :]
        blocks = [kv[block(j, C), :] for j in js]
        scores = [nt(query, b) * fox_scale + dall[:, block(j, C)] for j, b in zip(js, blocks)]
        if masked:
            q_at = lax.broadcasted_iota(jnp.int32, (R, C), 0) + i * R
            k_at = lax.broadcasted_iota(jnp.int32, (R, C), 1)
            scores = [jnp.where(k_at <= q_at, s, LOW) for s in scores]
        tops = [s[:, n * 128 : (n + 1) * 128] for s in scores for n in range(C // 128)]
        top = functools.reduce(jnp.maximum, tops)
        old = mx[rows, :]
        new = jnp.maximum(old, jnp.max(top, axis=1, keepdims=True))
        alpha = jnp.exp2(old - new)
        parts = [jnp.exp2(s - new) for s in tops]
        tot[rows, :] = alpha * tot[rows, :] + functools.reduce(jnp.add, parts)
        mx[rows, :] = new
        each = C // 128
        weighted = [
            nn(jnp.concatenate([p.astype(BF16) for p in parts[n * each : (n + 1) * each]], axis=1), b)
            for n, b in enumerate(blocks)
        ]
        acc[rows, :] = alpha * acc[rows, :] + functools.reduce(jnp.add, weighted)

    def inner(i):
        rows = block(i, Q)
        lanes = lax.broadcasted_iota(jnp.int32, (Q, 128), 1)
        query = jnp.where(jnp.logical_and(lanes >= 64, lanes < 96), rbuf[rows, :].astype(F32), 0.0).astype(BF16)
        keys = pltpu.roll(rbuf[...].astype(F32), 96, 1).astype(BF16)
        s = nt(query, keys)
        gap = lax.broadcasted_iota(jnp.int32, s.shape, 0) + i * Q - lax.broadcasted_iota(jnp.int32, s.shape, 1)
        within = jnp.where(gap >= 0, jnp.exp(jnp.maximum(gap, 0).astype(F32) * a), 0.0)
        high, low = split(s * key_scale * within)
        rin[rows, :] = nn(high, rbuf[...]) + nn(low, rbuf[...])

    def past(i, s):
        j = left_block(s)

        @pl.when(jnp.logical_and(z - s >= 0, j < 0))
        def _():
            attend(i, [z - s], False)

        @pl.when(j >= 0)
        def _():
            attend(i, [z - s, j], False)

    def finish_retention():
        span = float(C)
        far = z.astype(F32) * span

        def gather_state(j, total):
            gap = (z - 1 - j).astype(F32) * span
            return total + jnp.exp(jnp.zeros((16, 128), F32) + gap * a) * summ[j]

        packed = lax.fori_loop(0, z, gather_state, jnp.zeros((16, 128), F32))
        both = jnp.concatenate([packed, pltpu.roll(packed, 64, 1)], axis=0)
        start = jnp.where(is0, state[0], state[1])
        start = jnp.concatenate([start, jnp.zeros_like(start)], axis=1)
        lane32 = lax.broadcasted_iota(jnp.int32, (32, 128), 1)
        entering = jnp.where(lane32 < 64, both, 0.0) + jnp.exp(jnp.zeros((32, 128), F32) + far * a) * start
        entering = jnp.concatenate([jnp.zeros((64, 128), F32), entering, jnp.zeros((32, 128), F32)], axis=0)
        e_high, e_low = split(entering)
        hn = hng[...]
        hn = jnp.where(is0, hn, pltpu.roll(hn, 64, 1))

        def piece(i, carry):
            rows = block(i, Q)
            lanes = lax.broadcasted_iota(jnp.int32, (Q, 128), 1)
            place = (lax.broadcasted_iota(jnp.int32, (Q, 128), 0) + i * Q).astype(F32)
            leading = jnp.exp((place + 1.0) * a)
            query = rbuf[rows, :]
            raw = rin[rows, :] + (nn(query, e_high) + nn(query, e_low)) * leading
            raw = jnp.where(lanes < 64, raw, 0.0)
            center = jnp.where(lanes < 64, raw - jnp.sum(raw, axis=1, keepdims=True) * (1.0 / 64), 0.0)
            spread = jnp.sum(center * center, axis=1, keepdims=True) * (1.0 / 64)
            rin[rows, :] = center * lax.rsqrt(spread + EPS) * hn
            return carry

        lax.fori_loop(0, 4, piece, 0)

    def send_far(s):
        @pl.when(jnp.logical_and(early, s == (3 * z + 2) // 4 + 1))
        def _():
            pl.semaphore_wait(ready, 1)
            for k in (4, 0, 1, 2, 3):
                left_copy(k, jnp.minimum(z, H - 2), final).start()

    def attend_loop(s, carry):
        send_far(s)
        kv_step(4, s)
        for k in range(4):
            kv_step(k, s)
            idx = 4 * (s - 1) + k

            @pl.when(s == 1)
            def _():
                inner(k)

            if k == 0:

                @pl.when(s == H)
                def _():
                    finish_retention()

            if k % 2 == 1:

                @pl.when(s == 1)
                def _():
                    attend(k // 2, [z], True)

                @pl.when(s > 1)
                def _():
                    past(k // 2, s - 1)

            if k == 0:
                @pl.when(idx == H)
                def _():
                    ot_all[1]()

                @pl.when(idx == max(H, 2 * H - 4))
                def _():
                    ot_all[2]()

        return carry

    kv_start(4)
    lax.fori_loop(1, H + 1, attend_loop, 0)

    def last(i, carry):
        past(i, H)
        return carry

    lax.fori_loop(0, 2, last, 0)

    def finish(i, carry):
        rows = block(i, Q)
        lanes = lax.broadcasted_iota(jnp.int32, (Q, 128), 1)
        fox = acc[rows, :] / jnp.sum(tot[rows, :], axis=1, keepdims=True)
        mix[rows, :] = jnp.where(lanes < 64, rin[rows, :], fox).astype(BF16)
        return carry

    lax.fori_loop(0, 4, finish, 0)

    def mix_rows(core, member):
        return mix.at[pl.ds(pl.multiple_of(core * T + member * out_rows, out_rows), out_rows), :]

    here = mixall.at[x, :, pl.ds(pl.multiple_of(c * 128, 128), 128)]
    mix_sends = [remote(mix_rows(1 - c, x), here, mix_s.at[0], mix_r.at[0], sib)]
    for r in range(1, X):
        member = lax.rem(x + r, X)
        mix_sends.append(remote(mix_rows(c, member), here, mix_s.at[2 * r - 1], mix_r.at[2 * r - 1], peers[r - 1]))
        mix_sends.append(remote(mix_rows(1 - c, member), here, mix_s.at[2 * r], mix_r.at[2 * r], cross[r - 1]))
    for copy in mix_sends:
        copy.start()
    mixall[x, :, pl.ds(pl.multiple_of(c * 128, 128), 128)] = mix[
        pl.ds(pl.multiple_of(c * T + x * out_rows, out_rows), out_rows), :
    ]
    ot_all[3]()
    for copy in mix_sends:
        copy.wait_recv()

    tile = 256

    def project_out(n, carry):
        cols = pl.ds(pl.multiple_of(n * tile, tile), tile)
        total = jnp.zeros((out_rows, tile), F32)
        for g in range(X):
            total = total + nt(mixall[g], ot[g, cols, :]).astype(BF16).astype(F32)
        out[:, cols] = total.astype(BF16)
        return carry

    lax.fori_loop(0, D // tile, project_out, 0)

    for copy in mix_sends:
        copy.wait_send()
    tok_all[4]()
    ot_all[4]()
    for way in range(2):
        for reach in range(2):
            for k in range(4):
                w_copy(way, k, reach, z, 0).wait_send()
    for k in range(5):
        kv_end(k)


def local(Z, X, tokens, norm_gain, rqw, rkw, rvw, fqw, fkw, fvw, decay, state, hng, gates, row, fow):
    T = tokens.shape[0]
    C = 2 * T
    D = norm_gain.shape[0]
    H = Z // 2
    vm = pl.BlockSpec(memory_space=pltpu.VMEM)
    dma = pltpu.SemaphoreType.DMA
    in_specs = [vm] * 14
    in_specs[8] = pl.BlockSpec(memory_space=pltpu.SMEM)
    return pl.pallas_call(
        functools.partial(kernel, Z, X),
        out_shape=jax.ShapeDtypeStruct((T // X, D), BF16),
        in_specs=in_specs,
        out_specs=vm,
        scratch_shapes=[
            pltpu.VMEM((D, 256), BF16),
            pltpu.VMEM((D, 128), BF16),
            pltpu.VMEM((D // 2, 128), BF16),
            pltpu.VMEM((D, 128), BF16),
            pltpu.VMEM((rqw.shape[0], 256), BF16),
            pltpu.VMEM((rqw.shape[0], 128), BF16),
            pltpu.VMEM((rqw.shape[0] // 2, 128), BF16),
            pltpu.VMEM((2, T, D), BF16),
            pltpu.VMEM((C, D), BF16),
            pltpu.VMEM((Z * C, 128), BF16),
            pltpu.VMEM((C, 128), BF16),
            pltpu.VMEM((C, 128), BF16),
            pltpu.VMEM((C, 128), F32),
            pltpu.VMEM((Z, 16, 128), F32),
            pltpu.VMEM((1, Z * C), F32),
            pltpu.VMEM((C, 128), F32),
            pltpu.VMEM((C, 128), F32),
            pltpu.VMEM((C, 128), F32),
            pltpu.VMEM((X, D, 256), BF16),
            pltpu.VMEM((C, 128), BF16),
            pltpu.VMEM((X, T // X, 256), BF16),
            dma((3,)), dma((3,)),
            dma((X - 1,)), dma((X - 1,)), dma((X,)), dma((X,)), dma,
            dma((2, 2, 4)), dma((2, 2, H // 2, 4)),
            dma((2, 5)), dma((H, 5)), dma((H - 1, 5)), pltpu.SemaphoreType.REGULAR,
            dma((X - 1,)), dma((X - 1,)), dma((X,)), dma((X,)), dma,
            dma((2 * X - 1,)), dma((2 * X - 1,)),
        ],
        compiler_params=pltpu.CompilerParams(
            collective_id=0, has_side_effects=True, vmem_limit_bytes=56 * 1024 * 1024
        ),
    )(
        tokens, norm_gain.reshape(1, -1), rqw, rkw, rvw, fqw, fkw, fvw, decay, state,
        hng.reshape(1, -1), gates.T, row.T, fow.T,
    )


def solution(mesh):
    Z, X = mesh.shape["sp"] // 2, mesh.shape["tp"]
    return jax.shard_map(
        functools.partial(local, Z, X),
        mesh=mesh,
        in_specs=(
            P(("grp", "sp"), "tp"),
            P(),
            P("sp", "tp"),
            P("sp", "tp"),
            P("sp", "tp"),
            P("sp", "tp"),
            P("sp", "tp"),
            P("sp", "tp"),
            P("tp"),
            P(("grp", "tp"), None, None),
            P("tp"),
            P("grp", "tp"),
            P("tp", "sp"),
            P("tp", "sp"),
        ),
        out_specs=P(("grp", "sp", "tp"), None),
        check_vma=False,
    )
```

```python
import functools
import math

import jax
import jax.numpy as jnp
from jax import lax
from jax.experimental import pallas as pl
from jax.experimental.pallas import tpu as pltpu
from jax.sharding import PartitionSpec as P

MESH = pl.DeviceIdType.MESH
EPS = 1e-06
F32 = jnp.float32
BF16 = jnp.bfloat16
LOG2E = 1.4426950408889634
LOW = -3.0e38


def nt(a, b):
    return lax.dot_general(a, b, (((1,), (1,)), ((), ())), preferred_element_type=F32)


def nn(a, b):
    return jnp.dot(a, b, preferred_element_type=F32)


def split(a):
    high = a.astype(BF16)
    return high, (a - high.astype(F32)).astype(BF16)


def kernel(
    Z, X,
    tok, gain, rqw, rkw, rvw, fqw, fkw, fvw, dec, state, hng, gates, row, fow,
    out,
    wide_w, out_w, pack_w, query_w, send_w, send_o, send_p,
    tokall, normed, kv, qbuf, rbuf, rin, summ, dall, mx, tot, acc, ot, mix, mixall,
    swap_s, swap_r, tok_s, tok_r, tokc_s, tokc_r, tok_l, ws, wr, ks, kr, kl, ready,
    ot_s, ot_r, otc_s, otc_r, ot_l, mix_s, mix_r,
):
    sp = lax.axis_index("sp")
    x = lax.axis_index("tp")
    c = lax.rem(sp, 2)
    z = sp // 2
    H = Z // 2
    rows_w = rqw.shape[0]
    chip_w = 2 * rows_w
    D = gain.shape[1]
    T, feat = tok.shape
    C = 2 * T
    Q = C // 4
    out_rows = T // X
    is0 = c == 0

    def at_z(k):
        return {"sp": lax.rem(z + k + Z, Z) * 2 + c}

    hops = [(at_z(1), at_z(2)), (at_z(-1), at_z(-2))]
    sib = {"sp": z * 2 + 1 - c}
    final = {"sp": (Z - 1) * 2 + c}
    peers = [{"tp": lax.rem(x + r, X)} for r in range(1, X)]
    cross = [{"tp": lax.rem(x + r, X), "sp": z * 2 + 1 - c} for r in range(1, X)]

    def remote(src, dst, s, r, dev):
        return pltpu.make_async_remote_copy(
            src_ref=src, dst_ref=dst, send_sem=s, recv_sem=r, device_id=dev, device_id_type=MESH
        )

    def block(n, size):
        return pl.ds(pl.multiple_of(n * size, size), size)

    def head_block(h):
        def cut(ref):
            width = ref.shape[1] // 2
            return ref[:, h * width : (h + 1) * width].astype(F32)

        fq = cut(fqw)
        half = fq.shape[0] // 2
        return (
            jnp.concatenate([cut(fkw), cut(fvw), cut(rvw), cut(rqw), cut(rkw)], axis=1),
            jnp.concatenate([cut(row), cut(fow)], axis=1),
            jnp.concatenate([fq[:half], fq[half:]], axis=1),
        )

    first, second = head_block(0), head_block(1)
    own_rows = block(2 * z + c, rows_w)
    own_pack = block(2 * z + c, rows_w // 2)
    wide_w[own_rows, :] = jnp.where(is0, first[0], second[0]).astype(BF16)
    out_w[own_rows, :] = jnp.where(is0, first[1], second[1]).astype(BF16)
    pack_w[own_pack, :] = jnp.where(is0, first[2], second[2]).astype(BF16)
    send_w[...] = jnp.where(is0, second[0], first[0]).astype(BF16)
    send_o[...] = jnp.where(is0, second[1], first[1]).astype(BF16)
    send_p[...] = jnp.where(is0, second[2], first[2]).astype(BF16)

    barrier = pltpu.get_barrier_semaphore()
    partners = [hops[0][0], hops[0][1], hops[1][0], hops[1][1], sib] + peers + cross
    for dev in partners:
        pl.semaphore_signal(barrier, inc=1, device_id=dev, device_id_type=MESH)
    early = z <= H - 2
    is_last = z == Z - 1

    @pl.when(early)
    def _():
        pl.semaphore_signal(barrier, inc=1, device_id=final, device_id_type=MESH)

    pl.semaphore_wait(barrier, len(partners) + jnp.where(is_last, H - 1, 0))

    @pl.when(is_last)
    def _():
        for j in range(H - 1):
            pl.semaphore_signal(ready, inc=1, device_id={"sp": 2 * j + c}, device_id_type=MESH)

    swaps = [
        remote(send_w, wide_w.at[own_rows, :], swap_s.at[0], swap_r.at[0], sib),
        remote(send_o, out_w.at[own_rows, :], swap_s.at[1], swap_r.at[1], sib),
        remote(send_p, pack_w.at[own_pack, :], swap_s.at[2], swap_r.at[2], sib),
    ]
    for copy in swaps:
        copy.start()

    def source(r):
        return lax.rem(x - r + X, X)

    near = sorted({1, X - 1})

    def row_gather(src, at, s, r, cs, cr, local_sem):
        sends = [remote(src, at(x), s.at[n - 1], r.at[n - 1], peers[n - 1]) for n in near]
        over = [remote(src, at(x), cs.at[0], cr.at[0], sib)]
        over += [remote(at(source(n)), at(source(n)), cs.at[n], cr.at[n], sib) for n in near]
        own = pltpu.make_async_copy(src, at(x), local_sem)
        relays, later = [], []
        if X > 2:
            member = jnp.where(is0, source(1), source(X - 1))
            to = jnp.where(is0, lax.rem(x + 1, X), lax.rem(x + X - 1, X))
            relays = [remote(at(member), at(member), s.at[1], r.at[1], {"tp": to})]
            later = [remote(at(source(2)), at(source(2)), cs.at[2], cr.at[2], sib)]

        def begin():
            for copy in sends + over[:1]:
                copy.start()
            own.start()

        def middle():
            for copy in sends:
                copy.wait_recv()
            for copy in relays + over[1:]:
                copy.start()

        def close():
            own.wait()
            for copy in relays:
                copy.wait_recv()
            for copy in later:
                copy.start()

        def arrived():
            for copy in over + later:
                copy.wait_recv()

        def sent():
            for copy in sends + over + relays + later:
                copy.wait_send()

        return begin, middle, close, arrived, sent

    tok_all = row_gather(
        tok, lambda member: tokall.at[c, :, block(member, feat)], tok_s, tok_r, tokc_s, tokc_r, tok_l
    )
    tok_all[0]()

    nearby = gates[:, block(z, C)]
    gate_ref = jnp.where(is0, nearby[0:1, 0:128], nearby[1:2, 0:128])
    dall[...] = (gate_ref[:, 0:1] - jnp.where(is0, gates[0:1, :], gates[1:2, :])) * LOG2E

    for copy in swaps:
        copy.wait()

    def w_at(k, o):
        if k < 2:
            return wide_w.at[block(2 * o + k, rows_w), :]
        if k == 2:
            return pack_w.at[block(o, rows_w), :]
        return out_w.at[block(o, chip_w), :]

    def origin(way, d):
        return lax.rem(z - d + Z, Z) if way == 0 else lax.rem(z + d, Z)

    def w_copy(way, k, reach, o, t):
        return remote(
            w_at(k, o), w_at(k, o), ws.at[way, reach, k], wr.at[way, reach, t, k], hops[way][reach]
        )

    last_t = H // 2 - 1

    def w_step(t, k):
        for way in range(2):
            o = origin(way, 2 * t)

            @pl.when(t > 0)
            def _(way=way, o=o):
                w_copy(way, k, 1, o, t - 1).wait_recv()
                w_copy(way, k, 0, o, t).wait_send()

            w_copy(way, k, 0, o, t).start()
            mine = (k < 2) == (way == 0)

            def pass_two(way=way, o=o):
                @pl.when(t > 0)
                def _():
                    w_copy(way, k, 1, o, t).wait_send()

                w_copy(way, k, 1, o, t).start()

            if mine:
                pass_two()
            else:
                pl.when(t < last_t)(pass_two)

    pieces = 8
    P_rows = C // pieces
    rounds = last_t + 1
    w_total = 4 * rounds
    base = w_total // 2 + 1
    stride = 2
    inside = min(pieces, (w_total - base + stride - 1) // stride)

    def normalize(p):
        @pl.when(p == pieces // 2)
        def _():
            tok_all[3]()

        at = lax.rem(c * (pieces // 2) + p, pieces)
        half = at // (pieces // 2)
        values = tokall[half, block(lax.rem(at, pieces // 2), P_rows), :].astype(F32)
        scale = lax.rsqrt(jnp.mean(values * values, axis=1, keepdims=True) + EPS)
        normed[block(at, P_rows), :] = (values * scale * gain[...]).astype(BF16)

    def weights_loop(t, carry):
        for k in range(4):
            w_step(t, k)
            idx = 4 * t + k

            @pl.when(idx == w_total // 4)
            def _():
                tok_all[1]()

            @pl.when(idx == w_total // 2)
            def _():
                tok_all[2]()

            if k % 2 == 1:

                @pl.when(jnp.logical_and(idx >= base, idx < base + stride * inside))
                def _():
                    normalize((idx - base) // stride)

        return carry

    lax.fori_loop(0, rounds, weights_loop, 0)
    for p in range(inside, pieces):
        normalize(jnp.int32(p))

    def weights_end(chunks):
        def body(t, carry):
            for k in chunks:
                for way in range(2):
                    w_copy(way, k, 0, origin(way, 2 * t + 1), t).wait_recv()
            return carry

        lax.fori_loop(0, rounds, body, 0)
        for k in chunks:
            way = 0 if k < 2 else 1
            w_copy(way, k, 1, origin(way, H), last_t).wait_recv()

    weights_end((0, 1))

    def project_wide(i, carry):
        rows = block(i, Q)
        both = nn(normed[rows, :], wide_w[...]).astype(BF16)
        kv[block(z * 4 + i, Q), :] = both[:, :128]
        rbuf[rows, :] = both[:, 128:]
        return carry

    lax.fori_loop(0, 4, project_wide, 0)

    NK = 8

    def kv_at(k, o):
        return kv.at[block(o * NK + k, C // NK), :] if k < NK else summ.at[o]

    def right_copy(k, o, s):
        return remote(kv_at(k, o), kv_at(k, o), ks.at[0, k], kr.at[s - 1, k], hops[0][0])

    def left_copy(k, j, dev):
        return remote(kv_at(k, j), kv_at(k, j), ks.at[1, k], kl.at[j, k], dev)

    def kv_start(k):
        @pl.when(z < Z - 1)
        def _():
            right_copy(k, z, 1).start()

    def left_block(s, lag=4):
        return s - lag - (Z - 1 - z)

    def kv_step(k, s):
        @pl.when(jnp.logical_and(z - s >= 0, s <= H))
        def _():
            o = z - s
            right_copy(k, o, s).wait_recv()

            @pl.when(jnp.logical_and(z < Z - 1, s < H))
            def _():
                nxt = right_copy(k, o, s + 1)
                nxt.wait_send()
                nxt.start()

        j = left_block(s, 4 if k < NK else 2)

        @pl.when(j >= 0)
        def _():
            copy = left_copy(k, j, hops[1][0])
            copy.wait_recv()

            @pl.when(j <= z - H - 2)
            def _():
                @pl.when(j >= 1)
                def _():
                    copy.wait_send()

                copy.start()

    def kv_end(k):
        @pl.when(z < Z - 1)
        def _():
            right_copy(k, z, 1).wait_send()

        @pl.when(jnp.logical_or(early, z >= H + 2))
        def _():
            left_copy(k, 0, final).wait_send()

    for k in range(NK):
        kv_start(k)

    weights_end((2, 3))
    ot_all = row_gather(
        out_w, lambda member: ot.at[member, :, block(c, 128)], ot_s, ot_r, otc_s, otc_r, ot_l
    )
    ot_all[0]()

    lane_p = lax.broadcasted_iota(jnp.int32, (rows_w, 128), 1) < 64
    half_w = rows_w // 2

    def unpack(o, carry):
        packed = pack_w[block(o, rows_w), :].astype(F32)
        low = jnp.where(lane_p, packed, 0.0)
        high = jnp.where(lane_p, pltpu.roll(packed, 64, 1), 0.0)
        query_w[block(o, chip_w), :] = jnp.concatenate(
            [low[:half_w], high[:half_w], low[half_w:], high[half_w:]], axis=0
        ).astype(BF16)
        return carry

    lax.fori_loop(0, Z, unpack, 0, unroll=4)

    def project_query(i, carry):
        rows = block(i, Q)
        qbuf[rows, :] = nn(normed[rows, :], query_w[...]).astype(BF16)
        return carry

    lax.fori_loop(0, 4, project_query, 0)

    a = jnp.where(is0, dec[0], dec[1])
    key_size = rqw.shape[1] // 2
    key_scale = key_size ** (-0.5)
    sub = lax.broadcasted_iota(jnp.int32, (C, 128), 0)
    trail = jnp.exp((C - 1.0 - sub.astype(F32)) * a) * key_scale
    turned = (rbuf[...].astype(F32) * trail).T
    t_high, t_low = split(turned)
    grown = nn(t_high, rbuf[...]) + nn(t_low, rbuf[...])
    lane16 = lax.broadcasted_iota(jnp.int32, (16, 128), 1)
    summ[z] = jnp.where(lane16 < 64, grown[96:112, :], pltpu.roll(grown[112:128, :], 64, 1))

    mx[...] = jnp.full_like(mx, LOW)
    tot[...] = jnp.zeros_like(tot)
    acc[...] = jnp.zeros_like(acc)
    fox_scale = (fqw.shape[1] // 2) ** (-0.5) * LOG2E
    R = C // 2

    def attend(i, js, masked):
        rows = block(i, R)
        query = qbuf[rows, :]
        blocks = [kv[block(j, C), :] for j in js]
        scores = [nt(query, b) * fox_scale + dall[:, block(j, C)] for j, b in zip(js, blocks)]
        if masked:
            q_at = lax.broadcasted_iota(jnp.int32, (R, C), 0) + i * R
            k_at = lax.broadcasted_iota(jnp.int32, (R, C), 1)
            scores = [jnp.where(k_at <= q_at, s, LOW) for s in scores]
        tops = [s[:, n * 128 : (n + 1) * 128] for s in scores for n in range(C // 128)]
        top = functools.reduce(jnp.maximum, tops)
        old = mx[rows, :]
        new = jnp.maximum(old, jnp.max(top, axis=1, keepdims=True))
        alpha = jnp.exp2(old - new)
        parts = [jnp.exp2(s - new) for s in tops]
        tot[rows, :] = alpha * tot[rows, :] + functools.reduce(jnp.add, parts)
        mx[rows, :] = new
        each = C // 128
        weighted = [
            nn(jnp.concatenate([p.astype(BF16) for p in parts[n * each : (n + 1) * each]], axis=1), b)
            for n, b in enumerate(blocks)
        ]
        acc[rows, :] = alpha * acc[rows, :] + functools.reduce(jnp.add, weighted)

    def inner(i):
        rows = block(i, Q)
        lanes = lax.broadcasted_iota(jnp.int32, (Q, 128), 1)
        query = jnp.where(jnp.logical_and(lanes >= 64, lanes < 96), rbuf[rows, :].astype(F32), 0.0).astype(BF16)
        keys = pltpu.roll(rbuf[...].astype(F32), 96, 1).astype(BF16)
        s = nt(query, keys)
        gap = lax.broadcasted_iota(jnp.int32, s.shape, 0) + i * Q - lax.broadcasted_iota(jnp.int32, s.shape, 1)
        within = jnp.where(gap >= 0, jnp.exp(jnp.maximum(gap, 0).astype(F32) * a), 0.0)
        high, low = split(s * key_scale * within)
        rin[rows, :] = nn(high, rbuf[...]) + nn(low, rbuf[...])

    def past(i, s):
        j = left_block(s)

        right_too = jnp.logical_and(z - s >= 0, s <= H)

        @pl.when(jnp.logical_and(right_too, j < 0))
        def _():
            attend(i, [z - s], False)

        @pl.when(jnp.logical_and(right_too, j >= 0))
        def _():
            attend(i, [z - s, j], False)

        @pl.when(jnp.logical_and(j >= 0, s > H))
        def _():
            attend(i, [j], False)

    def finish_retention():
        span = float(C)
        far = z.astype(F32) * span

        def gather_state(j, total):
            gap = (z - 1 - j).astype(F32) * span
            return total + jnp.exp(jnp.zeros((16, 128), F32) + gap * a) * summ[j]

        packed = lax.fori_loop(0, z, gather_state, jnp.zeros((16, 128), F32))
        both = jnp.concatenate([packed, pltpu.roll(packed, 64, 1)], axis=0)
        start = jnp.where(is0, state[0], state[1])
        start = jnp.concatenate([start, jnp.zeros_like(start)], axis=1)
        lane32 = lax.broadcasted_iota(jnp.int32, (32, 128), 1)
        entering = jnp.where(lane32 < 64, both, 0.0) + jnp.exp(jnp.zeros((32, 128), F32) + far * a) * start
        entering = jnp.concatenate([jnp.zeros((64, 128), F32), entering, jnp.zeros((32, 128), F32)], axis=0)
        e_high, e_low = split(entering)
        hn = hng[...]
        hn = jnp.where(is0, hn, pltpu.roll(hn, 64, 1))

        def piece(i, carry):
            rows = block(i, Q)
            lanes = lax.broadcasted_iota(jnp.int32, (Q, 128), 1)
            place = (lax.broadcasted_iota(jnp.int32, (Q, 128), 0) + i * Q).astype(F32)
            leading = jnp.exp((place + 1.0) * a)
            query = rbuf[rows, :]
            raw = rin[rows, :] + (nn(query, e_high) + nn(query, e_low)) * leading
            raw = jnp.where(lanes < 64, raw, 0.0)
            center = jnp.where(lanes < 64, raw - jnp.sum(raw, axis=1, keepdims=True) * (1.0 / 64), 0.0)
            spread = jnp.sum(center * center, axis=1, keepdims=True) * (1.0 / 64)
            rin[rows, :] = center * lax.rsqrt(spread + EPS) * hn
            return carry

        lax.fori_loop(0, 4, piece, 0)

    def send_far(ks_now):
        for k in ks_now:
            left_copy(k, jnp.minimum(z, H - 2), final).start()

    pace = (29 * z) // 4 + jnp.where(z > 0, NK // 2, 0)

    def attend_loop(s, carry):
        @pl.when(s <= H)
        def _():
            kv_step(NK, s)

        for k in range(NK):
            kv_step(k, s)

            @pl.when(jnp.logical_and(early, NK * (s - 1) + k == pace))
            def _():
                send_far(range(NK))

            if k % 2 == 0:

                @pl.when(s == 1)
                def _():
                    inner(k // 2)

            if k == 0:

                @pl.when(s == H)
                def _():
                    finish_retention()

                @pl.when(s == H // 4 + 1)
                def _():
                    ot_all[1]()

                @pl.when(s == max(H // 4 + 1, H // 2))
                def _():
                    ot_all[2]()

            if k % 4 == 3:

                @pl.when(s == 1)
                def _():
                    attend(k // 4, [z], True)

                @pl.when(s > 1)
                def _():
                    past(k // 4, s - 1)

        return carry

    kv_start(NK)

    @pl.when(early)
    def _():
        pl.semaphore_wait(ready, 1)
        send_far([NK])

    lax.fori_loop(1, H + 3, attend_loop, 0)

    @pl.when(left_block(H + 2) >= 0)
    def _():
        def last(i, carry):
            attend(i, [left_block(H + 2)], False)
            return carry

        lax.fori_loop(0, 2, last, 0)


    def finish(i, carry):
        rows = block(i, Q)
        lanes = lax.broadcasted_iota(jnp.int32, (Q, 128), 1)
        fox = acc[rows, :] / jnp.sum(tot[rows, :], axis=1, keepdims=True)
        mix[rows, :] = jnp.where(lanes < 64, rin[rows, :], fox).astype(BF16)
        return carry

    lax.fori_loop(0, 4, finish, 0)

    def mix_rows(core, member):
        return mix.at[pl.ds(pl.multiple_of(core * T + member * out_rows, out_rows), out_rows), :]

    here = mixall.at[x, :, pl.ds(pl.multiple_of(c * 128, 128), 128)]
    mix_sends = [remote(mix_rows(1 - c, x), here, mix_s.at[0], mix_r.at[0], sib)]
    for r in range(1, X):
        member = lax.rem(x + r, X)
        mix_sends.append(remote(mix_rows(c, member), here, mix_s.at[2 * r - 1], mix_r.at[2 * r - 1], peers[r - 1]))
        mix_sends.append(remote(mix_rows(1 - c, member), here, mix_s.at[2 * r], mix_r.at[2 * r], cross[r - 1]))
    for copy in mix_sends:
        copy.start()
    mixall[x, :, pl.ds(pl.multiple_of(c * 128, 128), 128)] = mix[
        pl.ds(pl.multiple_of(c * T + x * out_rows, out_rows), out_rows), :
    ]
    ot_all[3]()
    for copy in mix_sends:
        copy.wait_recv()

    tile = 256

    def project_out(n, carry):
        cols = pl.ds(pl.multiple_of(n * tile, tile), tile)
        total = jnp.zeros((out_rows, tile), F32)
        for g in range(X):
            total = total + nt(mixall[g], ot[g, cols, :]).astype(BF16).astype(F32)
        out[:, cols] = total.astype(BF16)
        return carry

    lax.fori_loop(0, D // tile, project_out, 0)

    for copy in mix_sends:
        copy.wait_send()
    tok_all[4]()
    ot_all[4]()
    for way in range(2):
        for reach in range(2):
            for k in range(4):
                w_copy(way, k, reach, z, 0).wait_send()
    for k in range(NK + 1):
        kv_end(k)


def local(Z, X, tokens, norm_gain, rqw, rkw, rvw, fqw, fkw, fvw, decay, state, hng, gates, row, fow):
    T = tokens.shape[0]
    C = 2 * T
    D = norm_gain.shape[0]
    H = Z // 2
    vm = pl.BlockSpec(memory_space=pltpu.VMEM)
    dma = pltpu.SemaphoreType.DMA
    in_specs = [vm] * 14
    in_specs[8] = pl.BlockSpec(memory_space=pltpu.SMEM)
    return pl.pallas_call(
        functools.partial(kernel, Z, X),
        out_shape=jax.ShapeDtypeStruct((T // X, D), BF16),
        in_specs=in_specs,
        out_specs=vm,
        scratch_shapes=[
            pltpu.VMEM((D, 256), BF16),
            pltpu.VMEM((D, 128), BF16),
            pltpu.VMEM((D // 2, 128), BF16),
            pltpu.VMEM((D, 128), BF16),
            pltpu.VMEM((rqw.shape[0], 256), BF16),
            pltpu.VMEM((rqw.shape[0], 128), BF16),
            pltpu.VMEM((rqw.shape[0] // 2, 128), BF16),
            pltpu.VMEM((2, T, D), BF16),
            pltpu.VMEM((C, D), BF16),
            pltpu.VMEM((Z * C, 128), BF16),
            pltpu.VMEM((C, 128), BF16),
            pltpu.VMEM((C, 128), BF16),
            pltpu.VMEM((C, 128), F32),
            pltpu.VMEM((Z, 16, 128), F32),
            pltpu.VMEM((1, Z * C), F32),
            pltpu.VMEM((C, 128), F32),
            pltpu.VMEM((C, 128), F32),
            pltpu.VMEM((C, 128), F32),
            pltpu.VMEM((X, D, 256), BF16),
            pltpu.VMEM((C, 128), BF16),
            pltpu.VMEM((X, T // X, 256), BF16),
            dma((3,)), dma((3,)),
            dma((X - 1,)), dma((X - 1,)), dma((X,)), dma((X,)), dma,
            dma((2, 2, 4)), dma((2, 2, H // 2, 4)),
            dma((2, 9)), dma((H, 9)), dma((H - 1, 9)), pltpu.SemaphoreType.REGULAR,
            dma((X - 1,)), dma((X - 1,)), dma((X,)), dma((X,)), dma,
            dma((2 * X - 1,)), dma((2 * X - 1,)),
        ],
        compiler_params=pltpu.CompilerParams(
            collective_id=0, has_side_effects=True, vmem_limit_bytes=56 * 1024 * 1024
        ),
    )(
        tokens, norm_gain.reshape(1, -1), rqw, rkw, rvw, fqw, fkw, fvw, decay, state,
        hng.reshape(1, -1), gates.T, row.T, fow.T,
    )


def solution(mesh):
    Z, X = mesh.shape["sp"] // 2, mesh.shape["tp"]
    return jax.shard_map(
        functools.partial(local, Z, X),
        mesh=mesh,
        in_specs=(
            P(("grp", "sp"), "tp"),
            P(),
            P("sp", "tp"),
            P("sp", "tp"),
            P("sp", "tp"),
            P("sp", "tp"),
            P("sp", "tp"),
            P("sp", "tp"),
            P("tp"),
            P(("grp", "tp"), None, None),
            P("tp"),
            P("grp", "tp"),
            P("tp", "sp"),
            P("tp", "sp"),
        ),
        out_specs=P(("grp", "sp", "tp"), None),
        check_vma=False,
    )
```

```python
import functools
import math

import jax
import jax.numpy as jnp
from jax import lax
from jax.experimental import pallas as pl
from jax.experimental.pallas import tpu as pltpu
from jax.sharding import PartitionSpec as P

MESH = pl.DeviceIdType.MESH
EPS = 1e-06
F32 = jnp.float32
BF16 = jnp.bfloat16
LOG2E = 1.4426950408889634
LOW = -3.0e38


def nt(a, b):
    return lax.dot_general(a, b, (((1,), (1,)), ((), ())), preferred_element_type=F32)


def nn(a, b):
    return jnp.dot(a, b, preferred_element_type=F32)


def split(a):
    high = a.astype(BF16)
    return high, (a - high.astype(F32)).astype(BF16)


def kernel(
    Z, X,
    tok, gain, rqw, rkw, rvw, fqw, fkw, fvw, dec, state, hng, gates, row, fow,
    out,
    wide_w, out_w, pack_w, query_w, send_w, send_o, send_p,
    tokall, normed, kv, qbuf, rbuf, rin, summ, dall, mx, tot, acc, ot, mix, mixall,
    swap_s, swap_r, tok_s, tok_r, tokc_s, tokc_r, tok_l, ws, wr, ks, kr, kl, ready,
    ot_s, ot_r, otc_s, otc_r, ot_l, mix_s, mix_r,
):
    sp = lax.axis_index("sp")
    x = lax.axis_index("tp")
    c = lax.rem(sp, 2)
    z = sp // 2
    H = Z // 2
    rows_w = rqw.shape[0]
    chip_w = 2 * rows_w
    D = gain.shape[1]
    T, feat = tok.shape
    C = 2 * T
    Q = C // 4
    out_rows = T // X
    is0 = c == 0

    def at_z(k):
        return {"sp": lax.rem(z + k + Z, Z) * 2 + c}

    hops = [(at_z(1), at_z(2)), (at_z(-1), at_z(-2))]
    sib = {"sp": z * 2 + 1 - c}
    final = {"sp": (Z - 1) * 2 + c}
    peers = [{"tp": lax.rem(x + r, X)} for r in range(1, X)]
    cross = [{"tp": lax.rem(x + r, X), "sp": z * 2 + 1 - c} for r in range(1, X)]

    def remote(src, dst, s, r, dev):
        return pltpu.make_async_remote_copy(
            src_ref=src, dst_ref=dst, send_sem=s, recv_sem=r, device_id=dev, device_id_type=MESH
        )

    def block(n, size):
        return pl.ds(pl.multiple_of(n * size, size), size)

    def head_block(h):
        def cut(ref):
            width = ref.shape[1] // 2
            return ref[:, h * width : (h + 1) * width].astype(F32)

        fq = cut(fqw)
        half = fq.shape[0] // 2
        return (
            jnp.concatenate([cut(fkw), cut(fvw), cut(rvw), cut(rqw), cut(rkw)], axis=1),
            jnp.concatenate([cut(row), cut(fow)], axis=1),
            jnp.concatenate([fq[:half], fq[half:]], axis=1),
        )

    first, second = head_block(0), head_block(1)
    own_rows = block(2 * z + c, rows_w)
    own_pack = block(2 * z + c, rows_w // 2)
    wide_w[own_rows, :] = jnp.where(is0, first[0], second[0]).astype(BF16)
    out_w[own_rows, :] = jnp.where(is0, first[1], second[1]).astype(BF16)
    pack_w[own_pack, :] = jnp.where(is0, first[2], second[2]).astype(BF16)
    send_w[...] = jnp.where(is0, second[0], first[0]).astype(BF16)
    send_o[...] = jnp.where(is0, second[1], first[1]).astype(BF16)
    send_p[...] = jnp.where(is0, second[2], first[2]).astype(BF16)

    barrier = pltpu.get_barrier_semaphore()
    partners = [hops[0][0], hops[0][1], hops[1][0], hops[1][1], sib] + peers + cross
    for dev in partners:
        pl.semaphore_signal(barrier, inc=1, device_id=dev, device_id_type=MESH)
    early = z <= H - 2
    is_last = z == Z - 1

    @pl.when(early)
    def _():
        pl.semaphore_signal(barrier, inc=1, device_id=final, device_id_type=MESH)

    pl.semaphore_wait(barrier, len(partners) + jnp.where(is_last, H - 1, 0))

    @pl.when(is_last)
    def _():
        for j in range(H - 1):
            pl.semaphore_signal(ready, inc=1, device_id={"sp": 2 * j + c}, device_id_type=MESH)

    swaps = [
        remote(send_w, wide_w.at[own_rows, :], swap_s.at[0], swap_r.at[0], sib),
        remote(send_o, out_w.at[own_rows, :], swap_s.at[1], swap_r.at[1], sib),
        remote(send_p, pack_w.at[own_pack, :], swap_s.at[2], swap_r.at[2], sib),
    ]
    for copy in swaps:
        copy.start()

    def source(r):
        return lax.rem(x - r + X, X)

    near = sorted({1, X - 1})

    def row_gather(src, at, s, r, cs, cr, local_sem):
        sends = [remote(src, at(x), s.at[n - 1], r.at[n - 1], peers[n - 1]) for n in near]
        over = [remote(src, at(x), cs.at[0], cr.at[0], sib)]
        over += [remote(at(source(n)), at(source(n)), cs.at[n], cr.at[n], sib) for n in near]
        own = pltpu.make_async_copy(src, at(x), local_sem)
        relays, later = [], []
        if X > 2:
            member = jnp.where(is0, source(1), source(X - 1))
            to = jnp.where(is0, lax.rem(x + 1, X), lax.rem(x + X - 1, X))
            relays = [remote(at(member), at(member), s.at[1], r.at[1], {"tp": to})]
            later = [remote(at(source(2)), at(source(2)), cs.at[2], cr.at[2], sib)]

        def begin():
            for copy in sends + over[:1]:
                copy.start()
            own.start()

        def middle():
            for copy in sends:
                copy.wait_recv()
            for copy in relays + over[1:]:
                copy.start()

        def close():
            own.wait()
            for copy in relays:
                copy.wait_recv()
            for copy in later:
                copy.start()

        def arrived():
            for copy in over + later:
                copy.wait_recv()

        def sent():
            for copy in sends + over + relays + later:
                copy.wait_send()

        return begin, middle, close, arrived, sent

    tok_all = row_gather(
        tok, lambda member: tokall.at[c, :, block(member, feat)], tok_s, tok_r, tokc_s, tokc_r, tok_l
    )
    tok_all[0]()

    nearby = gates[:, block(z, C)]
    gate_ref = jnp.where(is0, nearby[0:1, 0:128], nearby[1:2, 0:128])
    dall[...] = (gate_ref[:, 0:1] - jnp.where(is0, gates[0:1, :], gates[1:2, :])) * LOG2E

    for copy in swaps:
        copy.wait()

    def w_at(k, o):
        if k < 2:
            return wide_w.at[block(2 * o + k, rows_w), :]
        if k == 2:
            return pack_w.at[block(o, rows_w), :]
        return out_w.at[block(o, chip_w), :]

    def origin(way, d):
        return lax.rem(z - d + Z, Z) if way == 0 else lax.rem(z + d, Z)

    def w_copy(way, k, reach, o, t):
        return remote(
            w_at(k, o), w_at(k, o), ws.at[way, reach, k], wr.at[way, reach, t, k], hops[way][reach]
        )

    last_t = H // 2 - 1

    def w_step(t, k):
        for way in range(2):
            o = origin(way, 2 * t)

            @pl.when(t > 0)
            def _(way=way, o=o):
                w_copy(way, k, 1, o, t - 1).wait_recv()
                w_copy(way, k, 0, o, t).wait_send()

            w_copy(way, k, 0, o, t).start()
            mine = (k < 2) == (way == 0)

            def pass_two(way=way, o=o):
                @pl.when(t > 0)
                def _():
                    w_copy(way, k, 1, o, t).wait_send()

                w_copy(way, k, 1, o, t).start()

            if mine:
                pass_two()
            else:
                pl.when(t < last_t)(pass_two)

    pieces = 8
    P_rows = C // pieces
    rounds = last_t + 1
    w_total = 4 * rounds
    base = w_total // 2 + 1
    stride = 2
    inside = min(pieces, (w_total - base + stride - 1) // stride)

    def normalize(p):
        @pl.when(p == pieces // 2)
        def _():
            tok_all[3]()

        at = lax.rem(c * (pieces // 2) + p, pieces)
        half = at // (pieces // 2)
        values = tokall[half, block(lax.rem(at, pieces // 2), P_rows), :].astype(F32)
        scale = lax.rsqrt(jnp.mean(values * values, axis=1, keepdims=True) + EPS)
        normed[block(at, P_rows), :] = (values * scale * gain[...]).astype(BF16)

    def weights_loop(t, carry):
        for k in range(4):
            w_step(t, k)
            idx = 4 * t + k

            @pl.when(idx == w_total // 4)
            def _():
                tok_all[1]()

            @pl.when(idx == w_total // 2)
            def _():
                tok_all[2]()

            if k % 2 == 1:

                @pl.when(jnp.logical_and(idx >= base, idx < base + stride * inside))
                def _():
                    normalize((idx - base) // stride)

        return carry

    lax.fori_loop(0, rounds, weights_loop, 0)
    for p in range(inside, pieces):
        normalize(jnp.int32(p))

    def weights_end(chunks):
        def body(t, carry):
            for k in chunks:
                for way in range(2):
                    w_copy(way, k, 0, origin(way, 2 * t + 1), t).wait_recv()
            return carry

        lax.fori_loop(0, rounds, body, 0)
        for k in chunks:
            way = 0 if k < 2 else 1
            w_copy(way, k, 1, origin(way, H), last_t).wait_recv()

    weights_end((0, 1))

    def project_wide(i, carry):
        rows = block(i, Q)
        both = nn(normed[rows, :], wide_w[...]).astype(BF16)
        kv[block(z * 4 + i, Q), :] = both[:, :128]
        rbuf[rows, :] = both[:, 128:]
        return carry

    lax.fori_loop(0, 4, project_wide, 0)

    NK = 8

    def kv_at(k, o):
        return kv.at[block(o * NK + k, C // NK), :] if k < NK else summ.at[o]

    def right_copy(k, o, s):
        return remote(kv_at(k, o), kv_at(k, o), ks.at[0, k], kr.at[s - 1, k], hops[0][0])

    def left_copy(k, j, dev):
        return remote(kv_at(k, j), kv_at(k, j), ks.at[1, k], kl.at[j, k], dev)

    def kv_start(k):
        @pl.when(z < Z - 1)
        def _():
            right_copy(k, z, 1).start()

    def left_block(s, lag=3):
        return s - lag - (Z - 1 - z)

    def kv_step(k, s):
        @pl.when(jnp.logical_and(z - s >= 0, s <= H))
        def _():
            o = z - s
            right_copy(k, o, s).wait_recv()

            @pl.when(jnp.logical_and(z < Z - 1, s < H))
            def _():
                nxt = right_copy(k, o, s + 1)
                nxt.wait_send()
                nxt.start()

        j = left_block(s, 3 if k < NK else 2)

        @pl.when(j >= 0)
        def _():
            copy = left_copy(k, j, hops[1][0])
            copy.wait_recv()

            @pl.when(j <= z - H - 2)
            def _():
                @pl.when(j >= 1)
                def _():
                    copy.wait_send()

                copy.start()

    def kv_end(k):
        @pl.when(z < Z - 1)
        def _():
            right_copy(k, z, 1).wait_send()

        @pl.when(jnp.logical_or(early, z >= H + 2))
        def _():
            left_copy(k, 0, final).wait_send()

    for k in range(NK):
        kv_start(k)

    weights_end((2, 3))
    ot_all = row_gather(
        out_w, lambda member: ot.at[member, :, block(c, 128)], ot_s, ot_r, otc_s, otc_r, ot_l
    )
    ot_all[0]()

    lane_p = lax.broadcasted_iota(jnp.int32, (rows_w, 128), 1) < 64
    half_w = rows_w // 2

    def unpack(o, carry):
        packed = pack_w[block(o, rows_w), :].astype(F32)
        low = jnp.where(lane_p, packed, 0.0)
        high = jnp.where(lane_p, pltpu.roll(packed, 64, 1), 0.0)
        query_w[block(o, chip_w), :] = jnp.concatenate(
            [low[:half_w], high[:half_w], low[half_w:], high[half_w:]], axis=0
        ).astype(BF16)
        return carry

    lax.fori_loop(0, Z, unpack, 0, unroll=4)

    def project_query(i, carry):
        rows = block(i, Q)
        qbuf[rows, :] = nn(normed[rows, :], query_w[...]).astype(BF16)
        return carry

    lax.fori_loop(0, 4, project_query, 0)

    a = jnp.where(is0, dec[0], dec[1])
    key_size = rqw.shape[1] // 2
    key_scale = key_size ** (-0.5)
    sub = lax.broadcasted_iota(jnp.int32, (C, 128), 0)
    trail = jnp.exp((C - 1.0 - sub.astype(F32)) * a) * key_scale
    turned = (rbuf[...].astype(F32) * trail).T
    t_high, t_low = split(turned)
    grown = nn(t_high, rbuf[...]) + nn(t_low, rbuf[...])
    lane16 = lax.broadcasted_iota(jnp.int32, (16, 128), 1)
    summ[z] = jnp.where(lane16 < 64, grown[96:112, :], pltpu.roll(grown[112:128, :], 64, 1))

    mx[...] = jnp.full_like(mx, LOW)
    tot[...] = jnp.zeros_like(tot)
    acc[...] = jnp.zeros_like(acc)
    fox_scale = (fqw.shape[1] // 2) ** (-0.5) * LOG2E
    R = C // 2

    def attend(i, js, masked):
        rows = block(i, R)
        query = qbuf[rows, :]
        blocks = [kv[block(j, C), :] for j in js]
        scores = [nt(query, b) * fox_scale + dall[:, block(j, C)] for j, b in zip(js, blocks)]
        if masked:
            q_at = lax.broadcasted_iota(jnp.int32, (R, C), 0) + i * R
            k_at = lax.broadcasted_iota(jnp.int32, (R, C), 1)
            scores = [jnp.where(k_at <= q_at, s, LOW) for s in scores]
        tops = [s[:, n * 128 : (n + 1) * 128] for s in scores for n in range(C // 128)]
        top = functools.reduce(jnp.maximum, tops)
        old = mx[rows, :]
        new = jnp.maximum(old, jnp.max(top, axis=1, keepdims=True))
        alpha = jnp.exp2(old - new)
        parts = [jnp.exp2(s - new) for s in tops]
        tot[rows, :] = alpha * tot[rows, :] + functools.reduce(jnp.add, parts)
        mx[rows, :] = new
        each = C // 128
        weighted = [
            nn(jnp.concatenate([p.astype(BF16) for p in parts[n * each : (n + 1) * each]], axis=1), b)
            for n, b in enumerate(blocks)
        ]
        acc[rows, :] = alpha * acc[rows, :] + functools.reduce(jnp.add, weighted)

    def inner(i):
        rows = block(i, Q)
        lanes = lax.broadcasted_iota(jnp.int32, (Q, 128), 1)
        query = jnp.where(jnp.logical_and(lanes >= 64, lanes < 96), rbuf[rows, :].astype(F32), 0.0).astype(BF16)
        keys = pltpu.roll(rbuf[...].astype(F32), 96, 1).astype(BF16)
        s = nt(query, keys)
        gap = lax.broadcasted_iota(jnp.int32, s.shape, 0) + i * Q - lax.broadcasted_iota(jnp.int32, s.shape, 1)
        within = jnp.where(gap >= 0, jnp.exp(jnp.maximum(gap, 0).astype(F32) * a), 0.0)
        high, low = split(s * key_scale * within)
        rin[rows, :] = nn(high, rbuf[...]) + nn(low, rbuf[...])

    def past(i, s):
        j = left_block(s)

        right_too = jnp.logical_and(z - s >= 0, s <= H)

        @pl.when(jnp.logical_and(right_too, j < 0))
        def _():
            attend(i, [z - s], False)

        @pl.when(jnp.logical_and(right_too, j >= 0))
        def _():
            attend(i, [z - s, j], False)

    def finish_retention():
        span = float(C)
        far = z.astype(F32) * span

        def gather_state(j, total):
            gap = (z - 1 - j).astype(F32) * span
            return total + jnp.exp(jnp.zeros((16, 128), F32) + gap * a) * summ[j]

        packed = lax.fori_loop(0, z, gather_state, jnp.zeros((16, 128), F32))
        both = jnp.concatenate([packed, pltpu.roll(packed, 64, 1)], axis=0)
        start = jnp.where(is0, state[0], state[1])
        start = jnp.concatenate([start, jnp.zeros_like(start)], axis=1)
        lane32 = lax.broadcasted_iota(jnp.int32, (32, 128), 1)
        entering = jnp.where(lane32 < 64, both, 0.0) + jnp.exp(jnp.zeros((32, 128), F32) + far * a) * start
        entering = jnp.concatenate([jnp.zeros((64, 128), F32), entering, jnp.zeros((32, 128), F32)], axis=0)
        e_high, e_low = split(entering)
        hn = hng[...]
        hn = jnp.where(is0, hn, pltpu.roll(hn, 64, 1))

        def piece(i, carry):
            rows = block(i, Q)
            lanes = lax.broadcasted_iota(jnp.int32, (Q, 128), 1)
            place = (lax.broadcasted_iota(jnp.int32, (Q, 128), 0) + i * Q).astype(F32)
            leading = jnp.exp((place + 1.0) * a)
            query = rbuf[rows, :]
            raw = rin[rows, :] + (nn(query, e_high) + nn(query, e_low)) * leading
            raw = jnp.where(lanes < 64, raw, 0.0)
            center = jnp.where(lanes < 64, raw - jnp.sum(raw, axis=1, keepdims=True) * (1.0 / 64), 0.0)
            spread = jnp.sum(center * center, axis=1, keepdims=True) * (1.0 / 64)
            rin[rows, :] = center * lax.rsqrt(spread + EPS) * hn
            return carry

        lax.fori_loop(0, 4, piece, 0)

    def send_far(ks_now):
        for k in ks_now:
            left_copy(k, jnp.minimum(z, H - 2), final).start()

    pace = (29 * z) // 4 + jnp.where(z > 0, NK // 2, 0)

    def attend_loop(s, carry):
        @pl.when(s <= H)
        def _():
            kv_step(NK, s)

        @pl.when(s == H + 1)
        def _():
            finish_retention()

        for k in range(NK):
            kv_step(k, s)

            @pl.when(jnp.logical_and(early, NK * (s - 1) + k == pace))
            def _():
                send_far(range(NK))

            if k % 2 == 0:

                @pl.when(s == 1)
                def _():
                    inner(k // 2)

            if k == 0:

                @pl.when(s == H // 4 + 1)
                def _():
                    ot_all[1]()

                @pl.when(s == max(H // 4 + 1, H // 2))
                def _():
                    ot_all[2]()

            if k % 4 == 3:

                @pl.when(s == 1)
                def _():
                    attend(k // 4, [z], True)

                @pl.when(s > 1)
                def _():
                    past(k // 4, s - 1)

        return carry

    kv_start(NK)

    @pl.when(early)
    def _():
        pl.semaphore_wait(ready, 1)
        send_far([NK])

    lax.fori_loop(1, H + 2, attend_loop, 0)

    @pl.when(left_block(H + 1) >= 0)
    def _():
        def last(i, carry):
            attend(i, [left_block(H + 1)], False)
            return carry

        lax.fori_loop(0, 2, last, 0, unroll=2)


    def finish(i, carry):
        rows = block(i, Q)
        lanes = lax.broadcasted_iota(jnp.int32, (Q, 128), 1)
        fox = acc[rows, :] / jnp.sum(tot[rows, :], axis=1, keepdims=True)
        mix[rows, :] = jnp.where(lanes < 64, rin[rows, :], fox).astype(BF16)
        return carry

    lax.fori_loop(0, 4, finish, 0)

    def mix_rows(core, member):
        return mix.at[pl.ds(pl.multiple_of(core * T + member * out_rows, out_rows), out_rows), :]

    here = mixall.at[x, :, pl.ds(pl.multiple_of(c * 128, 128), 128)]
    mix_sends = [remote(mix_rows(1 - c, x), here, mix_s.at[0], mix_r.at[0], sib)]
    for r in range(1, X):
        member = lax.rem(x + r, X)
        mix_sends.append(remote(mix_rows(c, member), here, mix_s.at[2 * r - 1], mix_r.at[2 * r - 1], peers[r - 1]))
        mix_sends.append(remote(mix_rows(1 - c, member), here, mix_s.at[2 * r], mix_r.at[2 * r], cross[r - 1]))
    for copy in mix_sends:
        copy.start()
    mixall[x, :, pl.ds(pl.multiple_of(c * 128, 128), 128)] = mix[
        pl.ds(pl.multiple_of(c * T + x * out_rows, out_rows), out_rows), :
    ]
    ot_all[3]()
    for copy in mix_sends:
        copy.wait_recv()

    tile = 256

    def project_out(n, carry):
        cols = pl.ds(pl.multiple_of(n * tile, tile), tile)
        total = jnp.zeros((out_rows, tile), F32)
        for g in range(X):
            total = total + nt(mixall[g], ot[g, cols, :]).astype(BF16).astype(F32)
        out[:, cols] = total.astype(BF16)
        return carry

    lax.fori_loop(0, D // tile, project_out, 0, unroll=2)

    for copy in mix_sends:
        copy.wait_send()
    tok_all[4]()
    ot_all[4]()
    for way in range(2):
        for reach in range(2):
            for k in range(4):
                w_copy(way, k, reach, z, 0).wait_send()
    for k in range(NK + 1):
        kv_end(k)


def local(Z, X, tokens, norm_gain, rqw, rkw, rvw, fqw, fkw, fvw, decay, state, hng, gates, row, fow):
    T = tokens.shape[0]
    C = 2 * T
    D = norm_gain.shape[0]
    H = Z // 2
    vm = pl.BlockSpec(memory_space=pltpu.VMEM)
    dma = pltpu.SemaphoreType.DMA
    in_specs = [vm] * 14
    in_specs[8] = pl.BlockSpec(memory_space=pltpu.SMEM)
    return pl.pallas_call(
        functools.partial(kernel, Z, X),
        out_shape=jax.ShapeDtypeStruct((T // X, D), BF16),
        in_specs=in_specs,
        out_specs=vm,
        scratch_shapes=[
            pltpu.VMEM((D, 256), BF16),
            pltpu.VMEM((D, 128), BF16),
            pltpu.VMEM((D // 2, 128), BF16),
            pltpu.VMEM((D, 128), BF16),
            pltpu.VMEM((rqw.shape[0], 256), BF16),
            pltpu.VMEM((rqw.shape[0], 128), BF16),
            pltpu.VMEM((rqw.shape[0] // 2, 128), BF16),
            pltpu.VMEM((2, T, D), BF16),
            pltpu.VMEM((C, D), BF16),
            pltpu.VMEM((Z * C, 128), BF16),
            pltpu.VMEM((C, 128), BF16),
            pltpu.VMEM((C, 128), BF16),
            pltpu.VMEM((C, 128), F32),
            pltpu.VMEM((Z, 16, 128), F32),
            pltpu.VMEM((1, Z * C), F32),
            pltpu.VMEM((C, 128), F32),
            pltpu.VMEM((C, 128), F32),
            pltpu.VMEM((C, 128), F32),
            pltpu.VMEM((X, D, 256), BF16),
            pltpu.VMEM((C, 128), BF16),
            pltpu.VMEM((X, T // X, 256), BF16),
            dma((3,)), dma((3,)),
            dma((X - 1,)), dma((X - 1,)), dma((X,)), dma((X,)), dma,
            dma((2, 2, 4)), dma((2, 2, H // 2, 4)),
            dma((2, 9)), dma((H, 9)), dma((H - 1, 9)), pltpu.SemaphoreType.REGULAR,
            dma((X - 1,)), dma((X - 1,)), dma((X,)), dma((X,)), dma,
            dma((2 * X - 1,)), dma((2 * X - 1,)),
        ],
        compiler_params=pltpu.CompilerParams(
            collective_id=0, has_side_effects=True, vmem_limit_bytes=56 * 1024 * 1024
        ),
    )(
        tokens, norm_gain.reshape(1, -1), rqw, rkw, rvw, fqw, fkw, fvw, decay, state,
        hng.reshape(1, -1), gates.T, row.T, fow.T,
    )


def solution(mesh):
    Z, X = mesh.shape["sp"] // 2, mesh.shape["tp"]
    return jax.shard_map(
        functools.partial(local, Z, X),
        mesh=mesh,
        in_specs=(
            P(("grp", "sp"), "tp"),
            P(),
            P("sp", "tp"),
            P("sp", "tp"),
            P("sp", "tp"),
            P("sp", "tp"),
            P("sp", "tp"),
            P("sp", "tp"),
            P("tp"),
            P(("grp", "tp"), None, None),
            P("tp"),
            P("grp", "tp"),
            P("tp", "sp"),
            P("tp", "sp"),
        ),
        out_specs=P(("grp", "sp", "tp"), None),
        check_vma=False,
    )
```

```python
import functools
import math

import jax
import jax.numpy as jnp
from jax import lax
from jax.experimental import pallas as pl
from jax.experimental.pallas import tpu as pltpu
from jax.sharding import PartitionSpec as P

MESH = pl.DeviceIdType.MESH
EPS = 1e-06
F32 = jnp.float32
BF16 = jnp.bfloat16
LOG2E = 1.4426950408889634
LOW = -3.0e38


def nt(a, b):
    return lax.dot_general(a, b, (((1,), (1,)), ((), ())), preferred_element_type=F32)


def nn(a, b):
    return jnp.dot(a, b, preferred_element_type=F32)


def split(a):
    high = a.astype(BF16)
    return high, (a - high.astype(F32)).astype(BF16)


def kernel(
    Z, X,
    tok, gain, rqw, rkw, rvw, fqw, fkw, fvw, dec, state, hng, gates, row, fow,
    out,
    wide_w, out_w, pack_w, query_w, send_w, send_o, send_p,
    tokall, normed, kv, qbuf, rbuf, rin, summ, dall, mx, tot, acc, ot, mix, mixall,
    swap_s, swap_r, tok_s, tok_r, tokc_s, tokc_r, tok_l, ws, wr, ys, yr, ks, kr, kl, ready,
    ot_s, ot_r, otc_s, otc_r, ot_l, mix_s, mix_r,
):
    sp = lax.axis_index("sp")
    x = lax.axis_index("tp")
    grp = lax.axis_index("grp")
    part = lax.rem(grp, 2)
    pair = {"grp": grp + 1 - 2 * part}
    c = lax.rem(sp, 2)
    z = sp // 2
    H = Z // 2
    rows_w = rqw.shape[0]
    chip_w = 2 * rows_w
    D = gain.shape[1]
    T, feat = tok.shape
    C = 2 * T
    Q = C // 4
    out_rows = T // X
    is0 = c == 0

    def at_z(k):
        return {"sp": lax.rem(z + k + Z, Z) * 2 + c}

    hops = [(at_z(1), at_z(2)), (at_z(-1), at_z(-2))]
    sib = {"sp": z * 2 + 1 - c}
    final = {"sp": (Z - 1) * 2 + c}
    peers = [{"tp": lax.rem(x + r, X)} for r in range(1, X)]
    cross = [{"tp": lax.rem(x + r, X), "sp": z * 2 + 1 - c} for r in range(1, X)]

    def remote(src, dst, s, r, dev):
        return pltpu.make_async_remote_copy(
            src_ref=src, dst_ref=dst, send_sem=s, recv_sem=r, device_id=dev, device_id_type=MESH
        )

    def block(n, size):
        return pl.ds(pl.multiple_of(n * size, size), size)

    def head_block(h):
        def cut(ref):
            width = ref.shape[1] // 2
            return ref[:, h * width : (h + 1) * width].astype(F32)

        fq = cut(fqw)
        half = fq.shape[0] // 2
        return (
            jnp.concatenate([cut(fkw), cut(fvw), cut(rvw), cut(rqw), cut(rkw)], axis=1),
            jnp.concatenate([cut(row), cut(fow)], axis=1),
            jnp.concatenate([fq[:half], fq[half:]], axis=1),
        )

    first, second = head_block(0), head_block(1)
    own_rows = block(2 * z + c, rows_w)
    own_pack = block(2 * z + c, rows_w // 2)
    wide_w[own_rows, :] = jnp.where(is0, first[0], second[0]).astype(BF16)
    out_w[own_rows, :] = jnp.where(is0, first[1], second[1]).astype(BF16)
    pack_w[own_pack, :] = jnp.where(is0, first[2], second[2]).astype(BF16)
    send_w[...] = jnp.where(is0, second[0], first[0]).astype(BF16)
    send_o[...] = jnp.where(is0, second[1], first[1]).astype(BF16)
    send_p[...] = jnp.where(is0, second[2], first[2]).astype(BF16)

    barrier = pltpu.get_barrier_semaphore()
    partners = [hops[0][0], hops[0][1], hops[1][0], hops[1][1], sib, pair] + peers + cross
    for dev in partners:
        pl.semaphore_signal(barrier, inc=1, device_id=dev, device_id_type=MESH)
    early = z <= H - 2
    is_last = z == Z - 1

    @pl.when(early)
    def _():
        pl.semaphore_signal(barrier, inc=1, device_id=final, device_id_type=MESH)

    pl.semaphore_wait(barrier, len(partners) + jnp.where(is_last, H - 1, 0))

    @pl.when(is_last)
    def _():
        for j in range(H - 1):
            pl.semaphore_signal(ready, inc=1, device_id={"sp": 2 * j + c}, device_id_type=MESH)

    swaps = [
        remote(send_w, wide_w.at[own_rows, :], swap_s.at[0], swap_r.at[0], sib),
        remote(send_o, out_w.at[own_rows, :], swap_s.at[1], swap_r.at[1], sib),
        remote(send_p, pack_w.at[own_pack, :], swap_s.at[2], swap_r.at[2], sib),
    ]
    for copy in swaps:
        copy.start()

    def source(r):
        return lax.rem(x - r + X, X)

    near = sorted({1, X - 1})

    def row_gather(src, at, s, r, cs, cr, local_sem):
        sends = [remote(src, at(x), s.at[n - 1], r.at[n - 1], peers[n - 1]) for n in near]
        over = [remote(src, at(x), cs.at[0], cr.at[0], sib)]
        over += [remote(at(source(n)), at(source(n)), cs.at[n], cr.at[n], sib) for n in near]
        own = pltpu.make_async_copy(src, at(x), local_sem)
        relays, later = [], []
        if X > 2:
            member = jnp.where(is0, source(1), source(X - 1))
            to = jnp.where(is0, lax.rem(x + 1, X), lax.rem(x + X - 1, X))
            relays = [remote(at(member), at(member), s.at[1], r.at[1], {"tp": to})]
            later = [remote(at(source(2)), at(source(2)), cs.at[2], cr.at[2], sib)]

        def begin():
            for copy in sends + over[:1]:
                copy.start()
            own.start()

        def middle():
            for copy in sends:
                copy.wait_recv()
            for copy in relays + over[1:]:
                copy.start()

        def close():
            own.wait()
            for copy in relays:
                copy.wait_recv()
            for copy in later:
                copy.start()

        def arrived():
            for copy in over + later:
                copy.wait_recv()

        def sent():
            for copy in sends + over + relays + later:
                copy.wait_send()

        return begin, middle, close, arrived, sent

    tok_all = row_gather(
        tok, lambda member: tokall.at[c, :, block(member, feat)], tok_s, tok_r, tokc_s, tokc_r, tok_l
    )
    tok_all[0]()

    nearby = gates[:, block(z, C)]
    gate_ref = jnp.where(is0, nearby[0:1, 0:128], nearby[1:2, 0:128])
    dall[...] = (gate_ref[:, 0:1] - jnp.where(is0, gates[0:1, :], gates[1:2, :])) * LOG2E

    for copy in swaps:
        copy.wait()

    def w_at(k, o, half):
        if k == 0:
            return wide_w.at[block(2 * o + half, rows_w), :]
        if k == 1:
            return out_w.at[block(2 * o + half, rows_w), :]
        return pack_w.at[block(2 * o + half, rows_w // 2), :]

    def origin(way, d):
        return lax.rem(z - d + Z, Z) if way == 0 else lax.rem(z + d, Z)

    def w_copy(way, k, reach, o, t):
        where = w_at(k, o, part)
        return remote(where, where, ws.at[way, reach, k], wr.at[way, reach, t, k], hops[way][reach])

    def y_copy(way, k, reach, t, half):
        where = w_at(k, origin(way, 2 * t + 1 + reach), half)
        return remote(where, where, ys.at[way, reach, k], yr.at[way, reach, t, k], pair)

    def hand_over(way, k, reach, t):
        w_copy(way, k, reach, origin(way, 2 * t + 1 + reach), t).wait_recv()
        copy = y_copy(way, k, reach, t, part)

        @pl.when(t > 0)
        def _():
            copy.wait_send()

        copy.start()

    last_t = H // 2 - 1

    def w_step(t, k):
        for way in range(2):
            o = origin(way, 2 * t)

            @pl.when(t > 0)
            def _(way=way, o=o):
                w_copy(way, k, 1, o, t - 1).wait_recv()
                w_copy(way, k, 0, o, t).wait_send()

            w_copy(way, k, 0, o, t).start()

            def pass_two(way=way, o=o):
                @pl.when(t > 0)
                def _():
                    w_copy(way, k, 1, o, t).wait_send()

                w_copy(way, k, 1, o, t).start()

            if (k < 1) == (way == 0):
                pass_two()
            else:
                pl.when(t < last_t)(pass_two)

        @pl.when(t > 0)
        def _():
            for way in range(2):
                copy = y_copy(way, k, 1, t - 1, part)

                @pl.when(t > 1)
                def _(copy=copy):
                    copy.wait_send()

                copy.start()
                hand_over(way, k, 0, t - 1)

    pieces = 8
    P_rows = C // pieces
    rounds = last_t + 1
    inside = 2 * (rounds - rounds // 2)

    def normalize(p):
        @pl.when(p == pieces // 2)
        def _():
            tok_all[3]()

        at = lax.rem(c * (pieces // 2) + p, pieces)
        half = at // (pieces // 2)
        values = tokall[half, block(lax.rem(at, pieces // 2), P_rows), :].astype(F32)
        scale = lax.rsqrt(jnp.mean(values * values, axis=1, keepdims=True) + EPS)
        normed[block(at, P_rows), :] = (values * scale * gain[...]).astype(BF16)

    def weights_loop(t, carry):
        for k in range(3):
            w_step(t, k)
            if k == 0:

                @pl.when(t == rounds // 4)
                def _():
                    tok_all[1]()

                @pl.when(t == rounds // 2)
                def _():
                    tok_all[2]()

            if k < 2:

                @pl.when(t >= rounds // 2)
                def _():
                    normalize(2 * (t - rounds // 2) + k)

        return carry

    lax.fori_loop(0, rounds, weights_loop, 0)

    def weights_end(k):
        mine = 0 if k < 1 else 1
        for way in range(2):
            hand_over(way, k, 0, jnp.int32(last_t))
        hand_over(mine, k, 1, jnp.int32(last_t))

    def weights_here(k):
        mine = 0 if k < 1 else 1

        def body(t, carry):
            for way in range(2):
                y_copy(way, k, 0, t, 1 - part).wait_recv()

                @pl.when(jnp.logical_or(t < last_t, way == mine))
                def _(way=way):
                    y_copy(way, k, 1, t, 1 - part).wait_recv()

            return carry

        lax.fori_loop(0, rounds, body, 0)

    for k in range(3):
        weights_end(k)
    for p in range(inside, pieces):
        normalize(jnp.int32(p))
    weights_here(0)

    def project_wide(i, carry):
        rows = block(i, Q)
        both = nn(normed[rows, :], wide_w[...]).astype(BF16)
        kv[block(z * 4 + i, Q), :] = both[:, :128]
        rbuf[rows, :] = both[:, 128:]
        return carry

    lax.fori_loop(0, 4, project_wide, 0)

    NK = 8

    def kv_at(k, o):
        return kv.at[block(o * NK + k, C // NK), :] if k < NK else summ.at[o]

    def right_copy(k, o, s):
        return remote(kv_at(k, o), kv_at(k, o), ks.at[0, k], kr.at[s - 1, k], hops[0][0])

    def left_copy(k, j, dev):
        return remote(kv_at(k, j), kv_at(k, j), ks.at[1, k], kl.at[j, k], dev)

    def kv_start(k):
        @pl.when(z < Z - 1)
        def _():
            right_copy(k, z, 1).start()

    def left_block(s, lag=3):
        return s - lag - (Z - 1 - z)

    def kv_step(k, s):
        @pl.when(jnp.logical_and(z - s >= 0, s <= H))
        def _():
            o = z - s
            right_copy(k, o, s).wait_recv()

            @pl.when(jnp.logical_and(z < Z - 1, s < H))
            def _():
                nxt = right_copy(k, o, s + 1)
                nxt.wait_send()
                nxt.start()

        j = left_block(s, 3 if k < NK else 2)

        @pl.when(j >= 0)
        def _():
            copy = left_copy(k, j, hops[1][0])
            copy.wait_recv()

            @pl.when(j <= z - H - 2)
            def _():
                @pl.when(j >= 1)
                def _():
                    copy.wait_send()

                copy.start()

    def kv_end(k):
        @pl.when(z < Z - 1)
        def _():
            right_copy(k, z, 1).wait_send()

        @pl.when(jnp.logical_or(early, z >= H + 2))
        def _():
            left_copy(k, 0, final).wait_send()

    for k in range(NK):
        kv_start(k)

    weights_here(1)
    ot_all = row_gather(
        out_w, lambda member: ot.at[member, :, block(c, 128)], ot_s, ot_r, otc_s, otc_r, ot_l
    )
    ot_all[0]()

    weights_here(2)

    lane_p = lax.broadcasted_iota(jnp.int32, (rows_w, 128), 1) < 64
    half_w = rows_w // 2

    def unpack(o, carry):
        packed = pack_w[block(o, rows_w), :].astype(F32)
        low = jnp.where(lane_p, packed, 0.0)
        high = jnp.where(lane_p, pltpu.roll(packed, 64, 1), 0.0)
        query_w[block(o, chip_w), :] = jnp.concatenate(
            [low[:half_w], high[:half_w], low[half_w:], high[half_w:]], axis=0
        ).astype(BF16)
        return carry

    lax.fori_loop(0, Z, unpack, 0, unroll=4)

    def project_query(i, carry):
        rows = block(i, Q)
        qbuf[rows, :] = nn(normed[rows, :], query_w[...]).astype(BF16)
        return carry

    lax.fori_loop(0, 4, project_query, 0)

    a = jnp.where(is0, dec[0], dec[1])
    key_size = rqw.shape[1] // 2
    key_scale = key_size ** (-0.5)
    sub = lax.broadcasted_iota(jnp.int32, (C, 128), 0)
    trail = jnp.exp((C - 1.0 - sub.astype(F32)) * a) * key_scale
    turned = (rbuf[...].astype(F32) * trail).T
    t_high, t_low = split(turned)
    grown = nn(t_high, rbuf[...]) + nn(t_low, rbuf[...])
    lane16 = lax.broadcasted_iota(jnp.int32, (16, 128), 1)
    summ[z] = jnp.where(lane16 < 64, grown[96:112, :], pltpu.roll(grown[112:128, :], 64, 1))

    mx[...] = jnp.full_like(mx, LOW)
    tot[...] = jnp.zeros_like(tot)
    acc[...] = jnp.zeros_like(acc)
    fox_scale = (fqw.shape[1] // 2) ** (-0.5) * LOG2E
    R = C // 2

    def attend(i, js, masked):
        rows = block(i, R)
        query = qbuf[rows, :]
        blocks = [kv[block(j, C), :] for j in js]
        scores = [nt(query, b) * fox_scale + dall[:, block(j, C)] for j, b in zip(js, blocks)]
        if masked:
            q_at = lax.broadcasted_iota(jnp.int32, (R, C), 0) + i * R
            k_at = lax.broadcasted_iota(jnp.int32, (R, C), 1)
            scores = [jnp.where(k_at <= q_at, s, LOW) for s in scores]
        tops = [s[:, n * 128 : (n + 1) * 128] for s in scores for n in range(C // 128)]
        top = functools.reduce(jnp.maximum, tops)
        old = mx[rows, :]
        new = jnp.maximum(old, jnp.max(top, axis=1, keepdims=True))
        alpha = jnp.exp2(old - new)
        parts = [jnp.exp2(s - new) for s in tops]
        tot[rows, :] = alpha * tot[rows, :] + functools.reduce(jnp.add, parts)
        mx[rows, :] = new
        each = C // 128
        weighted = [
            nn(jnp.concatenate([p.astype(BF16) for p in parts[n * each : (n + 1) * each]], axis=1), b)
            for n, b in enumerate(blocks)
        ]
        acc[rows, :] = alpha * acc[rows, :] + functools.reduce(jnp.add, weighted)

    def inner(i):
        rows = block(i, Q)
        lanes = lax.broadcasted_iota(jnp.int32, (Q, 128), 1)
        query = jnp.where(jnp.logical_and(lanes >= 64, lanes < 96), rbuf[rows, :].astype(F32), 0.0).astype(BF16)
        keys = pltpu.roll(rbuf[...].astype(F32), 96, 1).astype(BF16)
        s = nt(query, keys)
        gap = lax.broadcasted_iota(jnp.int32, s.shape, 0) + i * Q - lax.broadcasted_iota(jnp.int32, s.shape, 1)
        within = jnp.where(gap >= 0, jnp.exp(jnp.maximum(gap, 0).astype(F32) * a), 0.0)
        high, low = split(s * key_scale * within)
        rin[rows, :] = nn(high, rbuf[...]) + nn(low, rbuf[...])

    def past(i, s):
        j = left_block(s)

        right_too = jnp.logical_and(z - s >= 0, s <= H)

        @pl.when(jnp.logical_and(right_too, j < 0))
        def _():
            attend(i, [z - s], False)

        @pl.when(jnp.logical_and(right_too, j >= 0))
        def _():
            attend(i, [z - s, j], False)

    def finish_retention():
        span = float(C)
        far = z.astype(F32) * span

        def gather_state(j, total):
            gap = (z - 1 - j).astype(F32) * span
            return total + jnp.exp(jnp.zeros((16, 128), F32) + gap * a) * summ[j]

        packed = lax.fori_loop(0, z, gather_state, jnp.zeros((16, 128), F32))
        both = jnp.concatenate([packed, pltpu.roll(packed, 64, 1)], axis=0)
        start = jnp.where(is0, state[0], state[1])
        start = jnp.concatenate([start, jnp.zeros_like(start)], axis=1)
        lane32 = lax.broadcasted_iota(jnp.int32, (32, 128), 1)
        entering = jnp.where(lane32 < 64, both, 0.0) + jnp.exp(jnp.zeros((32, 128), F32) + far * a) * start
        entering = jnp.concatenate([jnp.zeros((64, 128), F32), entering, jnp.zeros((32, 128), F32)], axis=0)
        e_high, e_low = split(entering)
        hn = hng[...]
        hn = jnp.where(is0, hn, pltpu.roll(hn, 64, 1))

        def piece(i, carry):
            rows = block(i, Q)
            lanes = lax.broadcasted_iota(jnp.int32, (Q, 128), 1)
            place = (lax.broadcasted_iota(jnp.int32, (Q, 128), 0) + i * Q).astype(F32)
            leading = jnp.exp((place + 1.0) * a)
            query = rbuf[rows, :]
            raw = rin[rows, :] + (nn(query, e_high) + nn(query, e_low)) * leading
            raw = jnp.where(lanes < 64, raw, 0.0)
            center = jnp.where(lanes < 64, raw - jnp.sum(raw, axis=1, keepdims=True) * (1.0 / 64), 0.0)
            spread = jnp.sum(center * center, axis=1, keepdims=True) * (1.0 / 64)
            rin[rows, :] = center * lax.rsqrt(spread + EPS) * hn
            return carry

        lax.fori_loop(0, 4, piece, 0)

    def send_far(ks_now):
        for k in ks_now:
            left_copy(k, jnp.minimum(z, H - 2), final).start()

    pace = (29 * z) // 4 + jnp.where(z > 0, NK // 2, 0)

    def attend_loop(s, carry):
        @pl.when(s <= H)
        def _():
            kv_step(NK, s)

        @pl.when(s == H + 1)
        def _():
            finish_retention()

        for k in range(NK):
            kv_step(k, s)

            @pl.when(jnp.logical_and(early, NK * (s - 1) + k == pace))
            def _():
                send_far(range(NK))

            if k % 2 == 0:

                @pl.when(s == 1)
                def _():
                    inner(k // 2)

            if k == 0:

                @pl.when(s == H // 4 + 1)
                def _():
                    ot_all[1]()

                @pl.when(s == max(H // 4 + 1, H // 2))
                def _():
                    ot_all[2]()

            if k % 4 == 3:

                @pl.when(s == 1)
                def _():
                    attend(k // 4, [z], True)

                @pl.when(s > 1)
                def _():
                    past(k // 4, s - 1)

        return carry

    kv_start(NK)

    @pl.when(early)
    def _():
        pl.semaphore_wait(ready, 1)
        send_far([NK])

    lax.fori_loop(1, H + 2, attend_loop, 0)

    @pl.when(left_block(H + 1) >= 0)
    def _():
        def last(i, carry):
            attend(i, [left_block(H + 1)], False)
            return carry

        lax.fori_loop(0, 2, last, 0, unroll=2)


    def finish(i, carry):
        rows = block(i, Q)
        lanes = lax.broadcasted_iota(jnp.int32, (Q, 128), 1)
        fox = acc[rows, :] / jnp.sum(tot[rows, :], axis=1, keepdims=True)
        mix[rows, :] = jnp.where(lanes < 64, rin[rows, :], fox).astype(BF16)
        return carry

    lax.fori_loop(0, 4, finish, 0)

    def mix_rows(core, member):
        return mix.at[pl.ds(pl.multiple_of(core * T + member * out_rows, out_rows), out_rows), :]

    here = mixall.at[x, :, pl.ds(pl.multiple_of(c * 128, 128), 128)]
    mix_sends = [remote(mix_rows(1 - c, x), here, mix_s.at[0], mix_r.at[0], sib)]
    for r in range(1, X):
        member = lax.rem(x + r, X)
        mix_sends.append(remote(mix_rows(c, member), here, mix_s.at[2 * r - 1], mix_r.at[2 * r - 1], peers[r - 1]))
        mix_sends.append(remote(mix_rows(1 - c, member), here, mix_s.at[2 * r], mix_r.at[2 * r], cross[r - 1]))
    for copy in mix_sends:
        copy.start()
    mixall[x, :, pl.ds(pl.multiple_of(c * 128, 128), 128)] = mix[
        pl.ds(pl.multiple_of(c * T + x * out_rows, out_rows), out_rows), :
    ]
    ot_all[3]()
    for copy in mix_sends:
        copy.wait_recv()

    tile = 256

    def project_out(n, carry):
        cols = pl.ds(pl.multiple_of(n * tile, tile), tile)
        total = jnp.zeros((out_rows, tile), F32)
        for g in range(X):
            total = total + nt(mixall[g], ot[g, cols, :]).astype(BF16).astype(F32)
        out[:, cols] = total.astype(BF16)
        return carry

    lax.fori_loop(0, D // tile, project_out, 0, unroll=2)

    for copy in mix_sends:
        copy.wait_send()
    tok_all[4]()
    ot_all[4]()
    for way in range(2):
        for reach in range(2):
            for k in range(3):
                w_copy(way, k, reach, z, 0).wait_send()
                y_copy(way, k, reach, 0, part).wait_send()
    for k in range(NK + 1):
        kv_end(k)


def local(Z, X, tokens, norm_gain, rqw, rkw, rvw, fqw, fkw, fvw, decay, state, hng, gates, row, fow):
    T = tokens.shape[0]
    C = 2 * T
    D = norm_gain.shape[0]
    H = Z // 2
    vm = pl.BlockSpec(memory_space=pltpu.VMEM)
    dma = pltpu.SemaphoreType.DMA
    in_specs = [vm] * 14
    in_specs[8] = pl.BlockSpec(memory_space=pltpu.SMEM)
    return pl.pallas_call(
        functools.partial(kernel, Z, X),
        out_shape=jax.ShapeDtypeStruct((T // X, D), BF16),
        in_specs=in_specs,
        out_specs=vm,
        scratch_shapes=[
            pltpu.VMEM((D, 256), BF16),
            pltpu.VMEM((D, 128), BF16),
            pltpu.VMEM((D // 2, 128), BF16),
            pltpu.VMEM((D, 128), BF16),
            pltpu.VMEM((rqw.shape[0], 256), BF16),
            pltpu.VMEM((rqw.shape[0], 128), BF16),
            pltpu.VMEM((rqw.shape[0] // 2, 128), BF16),
            pltpu.VMEM((2, T, D), BF16),
            pltpu.VMEM((C, D), BF16),
            pltpu.VMEM((Z * C, 128), BF16),
            pltpu.VMEM((C, 128), BF16),
            pltpu.VMEM((C, 128), BF16),
            pltpu.VMEM((C, 128), F32),
            pltpu.VMEM((Z, 16, 128), F32),
            pltpu.VMEM((1, Z * C), F32),
            pltpu.VMEM((C, 128), F32),
            pltpu.VMEM((C, 128), F32),
            pltpu.VMEM((C, 128), F32),
            pltpu.VMEM((X, D, 256), BF16),
            pltpu.VMEM((C, 128), BF16),
            pltpu.VMEM((X, T // X, 256), BF16),
            dma((3,)), dma((3,)),
            dma((X - 1,)), dma((X - 1,)), dma((X,)), dma((X,)), dma,
            dma((2, 2, 3)), dma((2, 2, H // 2, 3)), dma((2, 2, 3)), dma((2, 2, H // 2, 3)),
            dma((2, 9)), dma((H, 9)), dma((H - 1, 9)), pltpu.SemaphoreType.REGULAR,
            dma((X - 1,)), dma((X - 1,)), dma((X,)), dma((X,)), dma,
            dma((2 * X - 1,)), dma((2 * X - 1,)),
        ],
        compiler_params=pltpu.CompilerParams(
            collective_id=0, has_side_effects=True, vmem_limit_bytes=56 * 1024 * 1024
        ),
    )(
        tokens, norm_gain.reshape(1, -1), rqw, rkw, rvw, fqw, fkw, fvw, decay, state,
        hng.reshape(1, -1), gates.T, row.T, fow.T,
    )


def solution(mesh):
    Z, X = mesh.shape["sp"] // 2, mesh.shape["tp"]
    return jax.shard_map(
        functools.partial(local, Z, X),
        mesh=mesh,
        in_specs=(
            P(("grp", "sp"), "tp"),
            P(),
            P("sp", "tp"),
            P("sp", "tp"),
            P("sp", "tp"),
            P("sp", "tp"),
            P("sp", "tp"),
            P("sp", "tp"),
            P("tp"),
            P(("grp", "tp"), None, None),
            P("tp"),
            P("grp", "tp"),
            P("tp", "sp"),
            P("tp", "sp"),
        ),
        out_specs=P(("grp", "sp", "tp"), None),
        check_vma=False,
    )
```

```python
import functools
import math

import jax
import jax.numpy as jnp
from jax import lax
from jax.experimental import pallas as pl
from jax.experimental.pallas import tpu as pltpu
from jax.sharding import PartitionSpec as P

MESH = pl.DeviceIdType.MESH
EPS = 1e-06
F32 = jnp.float32
BF16 = jnp.bfloat16
LOG2E = 1.4426950408889634
LOW = -3.0e38


def nt(a, b):
    return lax.dot_general(a, b, (((1,), (1,)), ((), ())), preferred_element_type=F32)


def nn(a, b):
    return jnp.dot(a, b, preferred_element_type=F32)


def split(a):
    high = a.astype(BF16)
    return high, (a - high.astype(F32)).astype(BF16)


def kernel(
    Z, X,
    tok, gain, rqw, rkw, rvw, fqw, fkw, fvw, dec, state, hng, gates, row, fow,
    out,
    wide_w, out_w, pack_w, query_w, send_w, send_o, send_p,
    tokall, normed, kv, qbuf, rbuf, rin, summ, dall, mx, tot, acc, ot, mix, mixall,
    swap_s, swap_r, tok_s, tok_r, tokc_s, tokc_r, tok_l, ws, wr, ks, kr, kl, ready,
    ot_s, ot_r, otc_s, otc_r, ot_l, mix_s, mix_r,
):
    sp = lax.axis_index("sp")
    x = lax.axis_index("tp")
    c = lax.rem(sp, 2)
    z = sp // 2
    H = Z // 2
    rows_w = rqw.shape[0]
    chip_w = 2 * rows_w
    D = gain.shape[1]
    T, feat = tok.shape
    C = 2 * T
    Q = C // 4
    out_rows = T // X
    is0 = c == 0

    def at_z(k):
        return {"sp": lax.rem(z + k + Z, Z) * 2 + c}

    hops = [(at_z(1), at_z(2)), (at_z(-1), at_z(-2))]
    sib = {"sp": z * 2 + 1 - c}
    final = {"sp": (Z - 1) * 2 + c}
    peers = [{"tp": lax.rem(x + r, X)} for r in range(1, X)]
    cross = [{"tp": lax.rem(x + r, X), "sp": z * 2 + 1 - c} for r in range(1, X)]

    def remote(src, dst, s, r, dev):
        return pltpu.make_async_remote_copy(
            src_ref=src, dst_ref=dst, send_sem=s, recv_sem=r, device_id=dev, device_id_type=MESH
        )

    def block(n, size):
        return pl.ds(pl.multiple_of(n * size, size), size)

    def head_block(h):
        def cut(ref):
            width = ref.shape[1] // 2
            return ref[:, h * width : (h + 1) * width].astype(F32)

        fq = cut(fqw)
        half = fq.shape[0] // 2
        return (
            jnp.concatenate([cut(fkw), cut(fvw), cut(rvw), cut(rqw), cut(rkw)], axis=1),
            jnp.concatenate([cut(row), cut(fow)], axis=1),
            jnp.concatenate([fq[:half], fq[half:]], axis=1),
        )

    first, second = head_block(0), head_block(1)
    own_rows = block(2 * z + c, rows_w)
    own_pack = block(2 * z + c, rows_w // 2)
    wide_w[own_rows, :] = jnp.where(is0, first[0], second[0]).astype(BF16)
    out_w[own_rows, :] = jnp.where(is0, first[1], second[1]).astype(BF16)
    pack_w[own_pack, :] = jnp.where(is0, first[2], second[2]).astype(BF16)
    send_w[...] = jnp.where(is0, second[0], first[0]).astype(BF16)
    send_o[...] = jnp.where(is0, second[1], first[1]).astype(BF16)
    send_p[...] = jnp.where(is0, second[2], first[2]).astype(BF16)

    barrier = pltpu.get_barrier_semaphore()
    partners = [hops[0][0], hops[0][1], hops[1][0], hops[1][1], sib] + peers + cross
    for dev in partners:
        pl.semaphore_signal(barrier, inc=1, device_id=dev, device_id_type=MESH)
    early = z <= H - 2
    is_last = z == Z - 1

    @pl.when(early)
    def _():
        pl.semaphore_signal(barrier, inc=1, device_id=final, device_id_type=MESH)

    pl.semaphore_wait(barrier, len(partners) + jnp.where(is_last, H - 1, 0))

    @pl.when(is_last)
    def _():
        for j in range(H - 1):
            pl.semaphore_signal(ready, inc=1, device_id={"sp": 2 * j + c}, device_id_type=MESH)

    swaps = [
        remote(send_w, wide_w.at[own_rows, :], swap_s.at[0], swap_r.at[0], sib),
        remote(send_o, out_w.at[own_rows, :], swap_s.at[1], swap_r.at[1], sib),
        remote(send_p, pack_w.at[own_pack, :], swap_s.at[2], swap_r.at[2], sib),
    ]
    for copy in swaps:
        copy.start()

    def source(r):
        return lax.rem(x - r + X, X)

    near = sorted({1, X - 1})

    def row_gather(src, at, s, r, cs, cr, local_sem):
        sends = [remote(src, at(x), s.at[n - 1], r.at[n - 1], peers[n - 1]) for n in near]
        over = [remote(src, at(x), cs.at[0], cr.at[0], sib)]
        over += [remote(at(source(n)), at(source(n)), cs.at[n], cr.at[n], sib) for n in near]
        own = pltpu.make_async_copy(src, at(x), local_sem)
        relays, later = [], []
        if X > 2:
            member = jnp.where(is0, source(1), source(X - 1))
            to = jnp.where(is0, lax.rem(x + 1, X), lax.rem(x + X - 1, X))
            relays = [remote(at(member), at(member), s.at[1], r.at[1], {"tp": to})]
            later = [remote(at(source(2)), at(source(2)), cs.at[2], cr.at[2], sib)]

        def begin():
            for copy in sends + over[:1]:
                copy.start()
            own.start()

        def middle():
            for copy in sends:
                copy.wait_recv()
            for copy in relays + over[1:]:
                copy.start()

        def close():
            own.wait()
            for copy in relays:
                copy.wait_recv()
            for copy in later:
                copy.start()

        def arrived():
            for copy in over + later:
                copy.wait_recv()

        def sent():
            for copy in sends + over + relays + later:
                copy.wait_send()

        return begin, middle, close, arrived, sent

    tok_all = row_gather(
        tok, lambda member: tokall.at[c, :, block(member, feat)], tok_s, tok_r, tokc_s, tokc_r, tok_l
    )
    tok_all[0]()

    nearby = gates[:, block(z, C)]
    gate_ref = jnp.where(is0, nearby[0:1, 0:128], nearby[1:2, 0:128])
    dall[...] = (gate_ref[:, 0:1] - jnp.where(is0, gates[0:1, :], gates[1:2, :])) * LOG2E

    for copy in swaps:
        copy.wait()

    def w_at(k, o):
        if k < 2:
            return wide_w.at[block(2 * o + k, rows_w), :]
        if k == 2:
            return pack_w.at[block(o, rows_w), :]
        return out_w.at[block(o, chip_w), :]

    def origin(way, d):
        return lax.rem(z - d + Z, Z) if way == 0 else lax.rem(z + d, Z)

    def w_copy(way, k, reach, o, t):
        return remote(
            w_at(k, o), w_at(k, o), ws.at[way, reach, k], wr.at[way, reach, t, k], hops[way][reach]
        )

    last_t = H // 2 - 1

    def w_step(t, k):
        for way in range(2):
            o = origin(way, 2 * t)

            @pl.when(t > 0)
            def _(way=way, o=o):
                w_copy(way, k, 1, o, t - 1).wait_recv()
                w_copy(way, k, 0, o, t).wait_send()

            w_copy(way, k, 0, o, t).start()
            mine = (k < 2) == (way == 0)

            def pass_two(way=way, o=o):
                @pl.when(t > 0)
                def _():
                    w_copy(way, k, 1, o, t).wait_send()

                w_copy(way, k, 1, o, t).start()

            if mine:
                pass_two()
            else:
                pl.when(t < last_t)(pass_two)

    pieces = 8
    P_rows = C // pieces
    rounds = last_t + 1
    w_total = 4 * rounds
    base = w_total // 2 + 1
    stride = 2
    inside = min(pieces, (w_total - base + stride - 1) // stride)

    def normalize(p):
        @pl.when(p == pieces // 2)
        def _():
            tok_all[3]()

        at = lax.rem(c * (pieces // 2) + p, pieces)
        half = at // (pieces // 2)
        values = tokall[half, block(lax.rem(at, pieces // 2), P_rows), :].astype(F32)
        scale = lax.rsqrt(jnp.mean(values * values, axis=1, keepdims=True) + EPS)
        normed[block(at, P_rows), :] = (values * scale * gain[...]).astype(BF16)

    def weights_loop(t, carry):
        for k in range(4):
            w_step(t, k)
            idx = 4 * t + k

            @pl.when(idx == w_total // 4)
            def _():
                tok_all[1]()

            @pl.when(idx == w_total // 2)
            def _():
                tok_all[2]()

            if k % 2 == 1:

                @pl.when(jnp.logical_and(idx >= base, idx < base + stride * inside))
                def _():
                    normalize((idx - base) // stride)

        return carry

    lax.fori_loop(0, rounds, weights_loop, 0)
    for p in range(inside, pieces):
        normalize(jnp.int32(p))

    def weights_end(chunks):
        def body(t, carry):
            for k in chunks:
                for way in range(2):
                    w_copy(way, k, 0, origin(way, 2 * t + 1), t).wait_recv()
            return carry

        lax.fori_loop(0, rounds, body, 0)
        for k in chunks:
            way = 0 if k < 2 else 1
            w_copy(way, k, 1, origin(way, H), last_t).wait_recv()

    weights_end((0, 1))

    def project_wide(i, carry):
        rows = block(i, Q)
        both = nn(normed[rows, :], wide_w[...]).astype(BF16)
        kv[block(z * 4 + i, Q), :] = both[:, :128]
        rbuf[rows, :] = both[:, 128:]
        return carry

    lax.fori_loop(0, 4, project_wide, 0, unroll=2)

    NK = 8

    def kv_at(k, o):
        return kv.at[block(o * NK + k, C // NK), :] if k < NK else summ.at[o]

    def right_copy(k, o, s):
        return remote(kv_at(k, o), kv_at(k, o), ks.at[0, k], kr.at[s - 1, k], hops[0][0])

    def left_copy(k, j, dev):
        return remote(kv_at(k, j), kv_at(k, j), ks.at[1, k], kl.at[j, k], dev)

    def kv_start(k):
        @pl.when(z < Z - 1)
        def _():
            right_copy(k, z, 1).start()

    def left_block(s, lag=3):
        return s - lag - (Z - 1 - z)

    def kv_step(k, s):
        @pl.when(jnp.logical_and(z - s >= 0, s <= H))
        def _():
            o = z - s
            right_copy(k, o, s).wait_recv()

            @pl.when(jnp.logical_and(z < Z - 1, s < H))
            def _():
                nxt = right_copy(k, o, s + 1)
                nxt.wait_send()
                nxt.start()

        j = left_block(s, 3 if k < NK else 2)

        @pl.when(j >= 0)
        def _():
            copy = left_copy(k, j, hops[1][0])
            copy.wait_recv()

            @pl.when(j <= z - H - 2)
            def _():
                @pl.when(j >= 1)
                def _():
                    copy.wait_send()

                copy.start()

    def kv_end(k):
        @pl.when(z < Z - 1)
        def _():
            right_copy(k, z, 1).wait_send()

        @pl.when(jnp.logical_or(early, z >= H + 2))
        def _():
            left_copy(k, 0, final).wait_send()

    for k in range(NK):
        kv_start(k)

    weights_end((2, 3))
    ot_all = row_gather(
        out_w, lambda member: ot.at[member, :, block(c, 128)], ot_s, ot_r, otc_s, otc_r, ot_l
    )
    ot_all[0]()

    lane_p = lax.broadcasted_iota(jnp.int32, (rows_w, 128), 1) < 64
    half_w = rows_w // 2

    def unpack(o, carry):
        packed = pack_w[block(o, rows_w), :].astype(F32)
        low = jnp.where(lane_p, packed, 0.0)
        high = jnp.where(lane_p, pltpu.roll(packed, 64, 1), 0.0)
        query_w[block(o, chip_w), :] = jnp.concatenate(
            [low[:half_w], high[:half_w], low[half_w:], high[half_w:]], axis=0
        ).astype(BF16)
        return carry

    lax.fori_loop(0, Z, unpack, 0, unroll=4)

    def project_query(i, carry):
        rows = block(i, Q)
        qbuf[rows, :] = nn(normed[rows, :], query_w[...]).astype(BF16)
        return carry

    lax.fori_loop(0, 4, project_query, 0, unroll=2)

    a = jnp.where(is0, dec[0], dec[1])
    key_size = rqw.shape[1] // 2
    key_scale = key_size ** (-0.5)
    sub = lax.broadcasted_iota(jnp.int32, (C, 128), 0)
    trail = jnp.exp((C - 1.0 - sub.astype(F32)) * a) * key_scale
    turned = (rbuf[...].astype(F32) * trail).T
    t_high, t_low = split(turned)
    grown = nn(t_high, rbuf[...]) + nn(t_low, rbuf[...])
    lane16 = lax.broadcasted_iota(jnp.int32, (16, 128), 1)
    summ[z] = jnp.where(lane16 < 64, grown[96:112, :], pltpu.roll(grown[112:128, :], 64, 1))

    mx[...] = jnp.full_like(mx, LOW)
    tot[...] = jnp.zeros_like(tot)
    acc[...] = jnp.zeros_like(acc)
    fox_scale = (fqw.shape[1] // 2) ** (-0.5) * LOG2E
    R = C // 2

    def attend(i, js, masked):
        rows = block(i, R)
        query = qbuf[rows, :]
        blocks = [kv[block(j, C), :] for j in js]
        scores = [nt(query, b) * fox_scale + dall[:, block(j, C)] for j, b in zip(js, blocks)]
        if masked:
            q_at = lax.broadcasted_iota(jnp.int32, (R, C), 0) + i * R
            k_at = lax.broadcasted_iota(jnp.int32, (R, C), 1)
            scores = [jnp.where(k_at <= q_at, s, LOW) for s in scores]
        tops = [s[:, n * 128 : (n + 1) * 128] for s in scores for n in range(C // 128)]
        top = functools.reduce(jnp.maximum, tops)
        old = mx[rows, :]
        new = jnp.maximum(old, jnp.max(top, axis=1, keepdims=True))
        alpha = jnp.exp2(old - new)
        parts = [jnp.exp2(s - new) for s in tops]
        tot[rows, :] = alpha * tot[rows, :] + functools.reduce(jnp.add, parts)
        mx[rows, :] = new
        each = C // 128
        weighted = [
            nn(jnp.concatenate([p.astype(BF16) for p in parts[n * each : (n + 1) * each]], axis=1), b)
            for n, b in enumerate(blocks)
        ]
        acc[rows, :] = alpha * acc[rows, :] + functools.reduce(jnp.add, weighted)

    def inner(i):
        rows = block(i, Q)
        lanes = lax.broadcasted_iota(jnp.int32, (Q, 128), 1)
        query = jnp.where(jnp.logical_and(lanes >= 64, lanes < 96), rbuf[rows, :].astype(F32), 0.0).astype(BF16)
        keys = pltpu.roll(rbuf[...].astype(F32), 96, 1).astype(BF16)
        s = nt(query, keys)
        gap = lax.broadcasted_iota(jnp.int32, s.shape, 0) + i * Q - lax.broadcasted_iota(jnp.int32, s.shape, 1)
        within = jnp.where(gap >= 0, jnp.exp(jnp.maximum(gap, 0).astype(F32) * a), 0.0)
        high, low = split(s * key_scale * within)
        rin[rows, :] = nn(high, rbuf[...]) + nn(low, rbuf[...])

    def past(i, s):
        j = left_block(s)

        right_too = jnp.logical_and(z - s >= 0, s <= H)

        @pl.when(jnp.logical_and(right_too, j < 0))
        def _():
            attend(i, [z - s], False)

        @pl.when(jnp.logical_and(right_too, j >= 0))
        def _():
            attend(i, [z - s, j], False)

    def finish_retention():
        span = float(C)
        far = z.astype(F32) * span

        def gather_state(j, total):
            gap = (z - 1 - j).astype(F32) * span
            return total + jnp.exp(jnp.zeros((16, 128), F32) + gap * a) * summ[j]

        packed = lax.fori_loop(0, z, gather_state, jnp.zeros((16, 128), F32))
        both = jnp.concatenate([packed, pltpu.roll(packed, 64, 1)], axis=0)
        start = jnp.where(is0, state[0], state[1])
        start = jnp.concatenate([start, jnp.zeros_like(start)], axis=1)
        lane32 = lax.broadcasted_iota(jnp.int32, (32, 128), 1)
        entering = jnp.where(lane32 < 64, both, 0.0) + jnp.exp(jnp.zeros((32, 128), F32) + far * a) * start
        entering = jnp.concatenate([jnp.zeros((64, 128), F32), entering, jnp.zeros((32, 128), F32)], axis=0)
        e_high, e_low = split(entering)
        hn = hng[...]
        hn = jnp.where(is0, hn, pltpu.roll(hn, 64, 1))

        def piece(i, carry):
            rows = block(i, Q)
            lanes = lax.broadcasted_iota(jnp.int32, (Q, 128), 1)
            place = (lax.broadcasted_iota(jnp.int32, (Q, 128), 0) + i * Q).astype(F32)
            leading = jnp.exp((place + 1.0) * a)
            query = rbuf[rows, :]
            raw = rin[rows, :] + (nn(query, e_high) + nn(query, e_low)) * leading
            raw = jnp.where(lanes < 64, raw, 0.0)
            center = jnp.where(lanes < 64, raw - jnp.sum(raw, axis=1, keepdims=True) * (1.0 / 64), 0.0)
            spread = jnp.sum(center * center, axis=1, keepdims=True) * (1.0 / 64)
            rin[rows, :] = center * lax.rsqrt(spread + EPS) * hn
            return carry

        lax.fori_loop(0, 4, piece, 0, unroll=2)

    def send_far(ks_now):
        for k in ks_now:
            left_copy(k, jnp.minimum(z, H - 2), final).start()

    pace = (29 * z) // 4 + jnp.where(z > 0, NK // 2, 0)

    def attend_loop(s, carry):
        @pl.when(s <= H)
        def _():
            kv_step(NK, s)

        @pl.when(s == H + 1)
        def _():
            finish_retention()

        for k in range(NK):
            kv_step(k, s)

            @pl.when(jnp.logical_and(early, NK * (s - 1) + k == pace))
            def _():
                send_far(range(NK))

            if k % 2 == 0:

                @pl.when(s == 1)
                def _():
                    inner(k // 2)

            if k == 0:

                @pl.when(s == H // 4 + 1)
                def _():
                    ot_all[1]()

                @pl.when(s == max(H // 4 + 1, H // 2))
                def _():
                    ot_all[2]()

            if k % 4 == 3:

                @pl.when(s == 1)
                def _():
                    attend(k // 4, [z], True)

                @pl.when(s > 1)
                def _():
                    past(k // 4, s - 1)

        return carry

    kv_start(NK)

    @pl.when(early)
    def _():
        pl.semaphore_wait(ready, 1)
        send_far([NK])

    lax.fori_loop(1, H + 2, attend_loop, 0)

    @pl.when(left_block(H + 1) >= 0)
    def _():
        def last(i, carry):
            attend(i, [left_block(H + 1)], False)
            return carry

        lax.fori_loop(0, 2, last, 0, unroll=2)


    def finish(i, carry):
        rows = block(i, Q)
        lanes = lax.broadcasted_iota(jnp.int32, (Q, 128), 1)
        fox = acc[rows, :] / jnp.sum(tot[rows, :], axis=1, keepdims=True)
        mix[rows, :] = jnp.where(lanes < 64, rin[rows, :], fox).astype(BF16)
        return carry

    lax.fori_loop(0, 4, finish, 0, unroll=2)

    def mix_rows(core, member):
        return mix.at[pl.ds(pl.multiple_of(core * T + member * out_rows, out_rows), out_rows), :]

    here = mixall.at[x, :, pl.ds(pl.multiple_of(c * 128, 128), 128)]
    mix_sends = [remote(mix_rows(1 - c, x), here, mix_s.at[0], mix_r.at[0], sib)]
    for r in range(1, X):
        member = lax.rem(x + r, X)
        mix_sends.append(remote(mix_rows(c, member), here, mix_s.at[2 * r - 1], mix_r.at[2 * r - 1], peers[r - 1]))
        mix_sends.append(remote(mix_rows(1 - c, member), here, mix_s.at[2 * r], mix_r.at[2 * r], cross[r - 1]))
    for copy in mix_sends:
        copy.start()
    mixall[x, :, pl.ds(pl.multiple_of(c * 128, 128), 128)] = mix[
        pl.ds(pl.multiple_of(c * T + x * out_rows, out_rows), out_rows), :
    ]
    ot_all[3]()
    for copy in mix_sends:
        copy.wait_recv()

    tile = 256

    def project_out(n, carry):
        cols = pl.ds(pl.multiple_of(n * tile, tile), tile)
        total = jnp.zeros((out_rows, tile), F32)
        for g in range(X):
            total = total + nt(mixall[g], ot[g, cols, :]).astype(BF16).astype(F32)
        out[:, cols] = total.astype(BF16)
        return carry

    lax.fori_loop(0, D // tile, project_out, 0, unroll=4)

    for copy in mix_sends:
        copy.wait_send()
    tok_all[4]()
    ot_all[4]()
    for way in range(2):
        for reach in range(2):
            for k in range(4):
                w_copy(way, k, reach, z, 0).wait_send()
    for k in range(NK + 1):
        kv_end(k)


def local(Z, X, tokens, norm_gain, rqw, rkw, rvw, fqw, fkw, fvw, decay, state, hng, gates, row, fow):
    T = tokens.shape[0]
    C = 2 * T
    D = norm_gain.shape[0]
    H = Z // 2
    vm = pl.BlockSpec(memory_space=pltpu.VMEM)
    dma = pltpu.SemaphoreType.DMA
    in_specs = [vm] * 14
    in_specs[8] = pl.BlockSpec(memory_space=pltpu.SMEM)
    return pl.pallas_call(
        functools.partial(kernel, Z, X),
        out_shape=jax.ShapeDtypeStruct((T // X, D), BF16),
        in_specs=in_specs,
        out_specs=vm,
        scratch_shapes=[
            pltpu.VMEM((D, 256), BF16),
            pltpu.VMEM((D, 128), BF16),
            pltpu.VMEM((D // 2, 128), BF16),
            pltpu.VMEM((D, 128), BF16),
            pltpu.VMEM((rqw.shape[0], 256), BF16),
            pltpu.VMEM((rqw.shape[0], 128), BF16),
            pltpu.VMEM((rqw.shape[0] // 2, 128), BF16),
            pltpu.VMEM((2, T, D), BF16),
            pltpu.VMEM((C, D), BF16),
            pltpu.VMEM((Z * C, 128), BF16),
            pltpu.VMEM((C, 128), BF16),
            pltpu.VMEM((C, 128), BF16),
            pltpu.VMEM((C, 128), F32),
            pltpu.VMEM((Z, 16, 128), F32),
            pltpu.VMEM((1, Z * C), F32),
            pltpu.VMEM((C, 128), F32),
            pltpu.VMEM((C, 128), F32),
            pltpu.VMEM((C, 128), F32),
            pltpu.VMEM((X, D, 256), BF16),
            pltpu.VMEM((C, 128), BF16),
            pltpu.VMEM((X, T // X, 256), BF16),
            dma((3,)), dma((3,)),
            dma((X - 1,)), dma((X - 1,)), dma((X,)), dma((X,)), dma,
            dma((2, 2, 4)), dma((2, 2, H // 2, 4)),
            dma((2, 9)), dma((H, 9)), dma((H - 1, 9)), pltpu.SemaphoreType.REGULAR,
            dma((X - 1,)), dma((X - 1,)), dma((X,)), dma((X,)), dma,
            dma((2 * X - 1,)), dma((2 * X - 1,)),
        ],
        compiler_params=pltpu.CompilerParams(
            collective_id=0, has_side_effects=True, vmem_limit_bytes=56 * 1024 * 1024
        ),
    )(
        tokens, norm_gain.reshape(1, -1), rqw, rkw, rvw, fqw, fkw, fvw, decay, state,
        hng.reshape(1, -1), gates.T, row.T, fow.T,
    )


def solution(mesh):
    Z, X = mesh.shape["sp"] // 2, mesh.shape["tp"]
    return jax.shard_map(
        functools.partial(local, Z, X),
        mesh=mesh,
        in_specs=(
            P(("grp", "sp"), "tp"),
            P(),
            P("sp", "tp"),
            P("sp", "tp"),
            P("sp", "tp"),
            P("sp", "tp"),
            P("sp", "tp"),
            P("sp", "tp"),
            P("tp"),
            P(("grp", "tp"), None, None),
            P("tp"),
            P("grp", "tp"),
            P("tp", "sp"),
            P("tp", "sp"),
        ),
        out_specs=P(("grp", "sp", "tp"), None),
        check_vma=False,
    )
```
